128 devices in a mesh: kv: 16 (over z, x), tp: 8 (over y, core).
Axes of the slice: x: 4, y: 4, z: 4, core: 2. Of those that a mesh axis runs over, the one named last changes fastest.
Arguments:
- activations: bfloat16 [384, 2048], P(None, ('kv', 'tp')), may hold values from -6 to 6
- latent_cache: bfloat16 [24, 32768, 288], P(None, 'kv'), may hold values from -6 to 6
- lengths: int32 [24], replicated, may hold values from 8192 to 32736, as said below
- accepted: int32 [24], replicated, may hold values from 0 to 16
- parents: int32 [24, 16], replicated, may hold values from -1 to 14, as said below
- w_query_down: bfloat16 [2048, 512], P(('kv', 'tp')), may hold values from -0.125 to 0.125
- w_key_down: bfloat16 [2048, 288], P(('kv', 'tp')), may hold values from -0.125 to 0.125
- gain_input: bfloat16 [2048], P(('kv', 'tp')), may hold values from 0.099609375 to 1.8984375
- gain_query: bfloat16 [512], replicated, may hold values from 0.099609375 to 1.8984375
- gain_key: bfloat16 [256], replicated, may hold values from 0.099609375 to 1.8984375
- w_query: bfloat16 [512, 16, 288], P(None, 'tp'), as said below
- w_value: bfloat16 [16, 256, 64], replicated, may hold values from -0.375 to 0.375
- w_out: bfloat16 [1024, 2048], P('tp', 'kv'), may hold values from -1 to 1, as said below
- gain_output: bfloat16 [2048], P('kv'), may hold values from 0.099609375 to 1.8984375
Outputs:
- mixed: bfloat16 [384, 2048], P(None, 'kv')
- new_cache: bfloat16 [24, 32768, 288], P(None, 'kv')
The draws below stay inside these ranges and needn't reach their ends.
Inputs may be any that keep to these rules, and one draw needn't show every extreme that they name: One sequence has lengths exactly 32736 and another exactly 8192; which ones varies. accepted is between 0 and 16, so the proposals' positions lie below 32768. `parents`: the parent of proposal i is -1 or a proposal with a smaller index; proposal 0 has parent -1; the proposals of exactly one sequence (which one varies) form a single chain; the other sequences' proposals form general trees. `w_query`: entries are normal with standard deviation (1536)^(-1/2) cut at six standard deviations; in the hidden draw the heads whose index is a multiple of 4 are 48 times larger. `w_out`: entries of order (1024)^(-1/2).
All inputs are finite; a program needn't handle non-finite values.
Results may differ from the reference program's by a relative error of at most 0.0096.
The reference program's roundings to bfloat16 on the way count: a program that leaves them out, or rounds other values in their place, can miss the bound.
Values may be sent and summed in bfloat16 or wider, within the bound.
No kernel may reach another device: no remote copies, remote signals or barrier semaphores. Data moves between devices by JAX's collectives and lax.ppermute only.
A program may use at most 192 MiB of HBM per device.

```python
import jax
import jax.numpy as jnp
from jax import lax

D = 2048
HEADS = 16
Q_RANK = 512
KV_RANK = 256
ROPE_DIM = 32
NOPE_DIM = 64
V_DIM = 64
PROPS = 16
SEQS = 24
POS_DEV = 2048
CACHE_LEN = 32768
ROWS = 384
N_KV = 16


def draw_w_query(key, part):
    spread = (3.0 * Q_RANK) ** (-0.5)
    drawn = jnp.clip(jax.random.normal(key, (Q_RANK, HEADS, KV_RANK + ROPE_DIM), jnp.float32), -6.0, 6.0) * spread
    return drawn.astype(jnp.bfloat16)


def draw_w_out(key, part):
    fan_width = HEADS * V_DIM
    spread = float(fan_width) ** (-0.5)
    base_key = jax.random.fold_in(key, 31)
    left_key = jax.random.fold_in(key, 32)
    right_key = jax.random.fold_in(key, 33)
    turn_key = jax.random.fold_in(key, 34)
    base = jnp.clip(jax.random.normal(base_key, (fan_width, D), jnp.float32), -4.0, 4.0) * spread
    left_signs = jnp.where(jax.random.bernoulli(left_key, 0.5, (fan_width,)), 1.0, -1.0).astype(jnp.float32)
    right_signs = jnp.where(jax.random.bernoulli(right_key, 0.5, (D,)), 1.0, -1.0).astype(jnp.float32)
    drawn = base + spread * left_signs[:, None] * right_signs[None, :]
    heading = jnp.where(jax.random.bernoulli(turn_key, 0.5, ()), 1.0, -1.0).astype(jnp.float32)
    column_pos = jnp.arange(D, dtype=jnp.float32) / float(D - 1) - 0.5
    column_scale = jnp.exp(heading * column_pos * jnp.log(3.0))
    drawn = drawn * column_scale[None, :]
    return drawn.astype(jnp.bfloat16)


def draw_lengths(key, part):
    value_key = jax.random.fold_in(key, 11)
    pick_key = jax.random.fold_in(key, 12)
    step_key = jax.random.fold_in(key, 13)
    drawn = jax.random.randint(value_key, (SEQS,), CACHE_LEN // 4, CACHE_LEN - 2 * PROPS + 1)
    seq_ids = jnp.arange(SEQS, dtype=jnp.int32)
    longest = jax.random.randint(pick_key, (), 0, SEQS)
    shortest = (longest + jax.random.randint(step_key, (), 1, SEQS)) % SEQS
    drawn = jnp.where(seq_ids == shortest, CACHE_LEN // 4, drawn)
    drawn = jnp.where(seq_ids == longest, CACHE_LEN - 2 * PROPS, drawn)
    return drawn.astype(jnp.int32)


def draw_parents(key, part):
    link_key = jax.random.fold_in(key, 21)
    pick_key = jax.random.fold_in(key, 22)
    slot_ids = jnp.arange(PROPS, dtype=jnp.int32)
    drawn = jax.random.randint(link_key, (SEQS, PROPS), -1, slot_ids[None, :])
    drawn = jnp.where(slot_ids[None, :] == 0, -1, drawn)
    chain_links = slot_ids - 1
    chained = jax.random.randint(pick_key, (), 0, SEQS)
    chain_seq = (jnp.arange(SEQS, dtype=jnp.int32) == chained)[:, None]
    return jnp.where(chain_seq, chain_links[None, :], drawn).astype(jnp.int32)


def set_ends(result, own_key, least, high):
    place = [jax.random.randint(jax.random.fold_in(own_key, axis), (), 0, length) for axis, length in enumerate(result.shape)]
    main_axis = result.shape.index(max(result.shape))
    neighbour = place[:main_axis] + [(place[main_axis] + 1) % result.shape[main_axis]] + place[main_axis + 1:]
    return result.at[tuple(place)].set(least).at[tuple(neighbour)].set(high)


def levels(own_key, shape, shards, smallest, top_value):
    def one(position, parts):
        draws = jax.random.uniform(jax.random.fold_in(jax.random.fold_in(own_key, 6), position), (parts,), jnp.float32, smallest / len(shards), top_value / len(shards))
        return jnp.repeat(jnp.exp(draws), shape[position] // parts).reshape((-1,) + (1,) * (len(shape) - position - 1))

    level = one(*shards[0])
    for cut in shards[1:]:
        level = level * one(*cut)
    return level


def bell_draw(own_key, shape, deviation, reach, pieces=(), held_as=jnp.bfloat16):
    values = jax.random.normal(own_key, shape, jnp.float32) * deviation
    if len(pieces) > 0:
        values = levels(own_key, shape, pieces, -0.22, 0.18) * values
    return jnp.clip(values, min=-reach, max=reach).astype(held_as)


def setup_inputs(seed: int = 0) -> dict:
    key_of = jax.random.split(jax.random.key(seed), 15)
    activations = bell_draw(key_of[0], (ROWS, D), 1.0, 6.0, ((1, 128),))
    latent_cache = bell_draw(key_of[1], (SEQS, CACHE_LEN, KV_RANK + ROPE_DIM), 1.0, 6.0, ((1, 16),))
    lengths = draw_lengths(jax.random.fold_in(key_of[14], 71), 0)
    accepted = set_ends(jax.random.randint(key_of[3], (SEQS,), 0, PROPS + 1), jax.random.fold_in(key_of[3], 1), 0, PROPS).astype(jnp.int32)
    parents = draw_parents(jax.random.fold_in(key_of[14], 71), 0)
    w_query_down = bell_draw(key_of[5], (D, Q_RANK), D ** -0.5, 0.125, ((0, 128),))
    w_key_down = bell_draw(key_of[6], (D, KV_RANK + ROPE_DIM), D ** -0.5, 0.125, ((0, 128),))
    gain_input = jnp.clip(1.0 + 0.18 * jax.random.normal(key_of[7], (D,), jnp.float32), 0.099609375, 1.8984375).astype(jnp.bfloat16)
    gain_query = jnp.clip(1.0 + 0.18 * jax.random.normal(key_of[8], (Q_RANK,), jnp.float32), 0.099609375, 1.8984375).astype(jnp.bfloat16)
    gain_key = jnp.clip(1.0 + 0.18 * jax.random.normal(key_of[9], (KV_RANK,), jnp.float32), 0.099609375, 1.8984375).astype(jnp.bfloat16)
    w_query = draw_w_query(jax.random.fold_in(key_of[14], 71), 0)
    w_value = bell_draw(key_of[11], (HEADS, KV_RANK, V_DIM), KV_RANK ** -0.5, 0.375)
    w_out = draw_w_out(jax.random.fold_in(key_of[14], 71), 0)
    gain_output = jnp.clip(1.0 + 0.18 * jax.random.normal(key_of[13], (D,), jnp.float32), 0.099609375, 1.8984375).astype(jnp.bfloat16)
    return {"activations": activations, "latent_cache": latent_cache, "lengths": lengths, "accepted": accepted, "parents": parents, "w_query_down": w_query_down, "w_key_down": w_key_down, "gain_input": gain_input, "gain_query": gain_query, "gain_key": gain_key, "w_query": w_query, "w_value": w_value, "w_out": w_out, "gain_output": gain_output}


epsilon = 1e-06
rope_base = 10000.0
score_after_mask = -1e+30

def rotate(component, places):
    half_width = component.shape[-1] // 2
    frequency = rope_base ** (-jnp.arange(half_width, dtype=jnp.float32) / half_width)
    angles = places.astype(jnp.float32)[:, None] * frequency[None, :]
    target_shape = (places.shape[0],) + (1,) * (component.ndim - 2) + (half_width,)
    cosine = jnp.cos(angles).reshape(target_shape)
    sine_part = jnp.sin(angles).reshape(target_shape)
    front_half = component[..., :half_width]
    back_half = component[..., half_width:]
    return jnp.concatenate([front_half * cosine - back_half * sine_part, back_half * cosine + front_half * sine_part], axis=-1)

def normalize(values, scales):
    return values * lax.rsqrt(lax.optimization_barrier(jnp.mean(values * values, axis=-1, keepdims=True)) + epsilon) * scales.astype(jnp.float32)

def ancestry(parents):
    seq_count, prop_count = parents.shape
    slot_ids = jnp.arange(prop_count, dtype=jnp.int32)
    parent_links = (parents[:, :, None] == slot_ids[None, None, :]).astype(jnp.float32)
    identity = jnp.broadcast_to(jnp.eye(prop_count, dtype=jnp.float32), parent_links.shape)
    reached = jnp.minimum(identity + parent_links, 1.0)
    for repeat in range((prop_count - 1).bit_length()):
        reached = jnp.minimum(jnp.einsum('sij,sjk->sik', reached, reached, precision=lax.Precision.HIGHEST), 1.0)
    depths = (lax.optimization_barrier(jnp.sum(reached, axis=-1)) - 1.0).astype(jnp.int32)
    return (reached, depths)

def partial_attend(queries, key_rows, slot_index, onehot, reached, w_value):
    score_scale = (NOPE_DIM + ROPE_DIM) ** (-0.5)
    ancestors = jnp.einsum('sij,snj->sin', reached, onehot, precision=lax.Precision.HIGHEST)
    visible = ((slot_index < 0)[:, None, :] | (ancestors > 0.5))[:, :, None, :]
    scores = jnp.einsum('siha,sna->sihn', queries.astype(jnp.float32), key_rows.astype(jnp.float32), precision=lax.Precision.HIGHEST) * score_scale
    masked = jnp.where(visible, scores, score_after_mask)
    maxima = lax.optimization_barrier(jnp.max(masked, axis=-1))
    weights = jnp.where(visible, jnp.exp(masked - maxima[..., None]), 0.0)
    totals = lax.optimization_barrier(jnp.sum(weights, axis=-1))
    rounded = lax.optimization_barrier(weights.astype(jnp.bfloat16))
    weighted = jnp.einsum('sihn,snk->sihk', rounded.astype(jnp.float32), key_rows[:, :, :KV_RANK].astype(jnp.float32), precision=lax.Precision.HIGHEST)
    value_fraction = lax.optimization_barrier((weighted / jnp.maximum(totals, 1.0)[..., None]).astype(jnp.bfloat16))
    values = jnp.einsum('siha,hav->sihv', value_fraction.astype(jnp.float32), w_value.astype(jnp.float32), precision=lax.Precision.HIGHEST).astype(jnp.bfloat16)
    return (maxima, totals, values)

def combine_parts(maxima, totals, values):
    largest = lax.optimization_barrier(jnp.max(maxima, axis=0))
    shares = totals * jnp.exp(maxima - largest[None])
    summed = lax.optimization_barrier(jnp.sum(shares[..., None] * values.astype(jnp.float32), axis=0))
    return summed / lax.optimization_barrier(jnp.sum(shares, axis=0))[..., None]

def location_rows(seq_cache, rows_of, anchor):
    return lax.dynamic_update_slice(seq_cache, rows_of, (anchor, jnp.int32(0)))

def reference(activations, latent_cache, lengths, accepted, parents, w_query_down, w_key_down, gain_input, gain_query, gain_key, w_query, w_value, w_out, gain_output):
    reached, depths = ancestry(parents)
    filled = lengths + accepted
    places = (filled[:, None] + depths).reshape(-1)
    as_float = activations.astype(jnp.float32)
    scaled = (as_float * gain_input.astype(jnp.float32)).astype(jnp.bfloat16)
    inverse = lax.rsqrt(lax.optimization_barrier(jnp.mean(as_float * as_float, axis=-1, keepdims=True)) + epsilon)
    query_raw = jnp.dot(scaled, w_query_down, preferred_element_type=jnp.float32) * inverse
    key_raw = jnp.dot(scaled, w_key_down, preferred_element_type=jnp.float32) * inverse
    query_low = normalize(query_raw, gain_query).astype(jnp.bfloat16)
    mapped_output = jnp.dot(query_low, w_query.reshape(Q_RANK, -1), preferred_element_type=jnp.float32)
    mapped_output = mapped_output.reshape(ROWS, HEADS, KV_RANK + ROPE_DIM)
    queries = jnp.concatenate([mapped_output[..., :KV_RANK], rotate(mapped_output[..., KV_RANK:], places)], axis=-1).astype(jnp.bfloat16)
    fresh_rows = jnp.concatenate([normalize(key_raw[:, :KV_RANK], gain_key), rotate(key_raw[:, KV_RANK:], places)], axis=-1).astype(jnp.bfloat16)
    fresh_block = fresh_rows.reshape(SEQS, PROPS, KV_RANK + ROPE_DIM)
    updated = jax.vmap(location_rows)(latent_cache, fresh_block, filled)
    queries = lax.optimization_barrier(queries).reshape(SEQS, PROPS, HEADS, KV_RANK + ROPE_DIM)
    keys_all = lax.optimization_barrier(updated)

    def one_block(index_block):
        anchor = index_block * POS_DEV
        key_rows = lax.dynamic_slice_in_dim(keys_all, anchor, POS_DEV, 1)
        locations_held = anchor + jnp.arange(POS_DEV, dtype=jnp.int32)
        slot_index = locations_held[None, :] - filled[:, None]
        onehot = (slot_index[:, :, None] == jnp.arange(PROPS, dtype=jnp.int32)[None, None, :]).astype(jnp.float32)
        return partial_attend(queries, key_rows, slot_index, onehot, reached, w_value)
    maxima, totals, values = lax.map(one_block, jnp.arange(N_KV, dtype=jnp.int32))
    values = lax.optimization_barrier(values)
    attended = combine_parts(maxima, totals, values).astype(jnp.bfloat16).reshape(ROWS, HEADS * V_DIM)
    mixed_raw = jnp.dot(attended, w_out, preferred_element_type=jnp.float32)
    mixed = normalize(mixed_raw, gain_output).astype(jnp.bfloat16)
    return (mixed, updated)
```

```python
import jax
import jax.numpy as jnp
from jax import lax
from jax.experimental import pallas as pl
from jax.experimental.pallas import tpu as pltpu
from jax.sharding import PartitionSpec as P


f32 = jnp.float32
bf16 = jnp.bfloat16

D = 2048
SEQS = 24
PROPS = 16
SPAN = 2048
ROPE_DIM = 32
LINES = 288
SCALE = 96.0 ** (-0.5)
EPS = 1e-06
ROPE_BASE = 10000.0
MASKED = -1e30
ALL = ("kv", "tp")
VMEM = pltpu.VMEM


def vmem_spec():
    return pl.BlockSpec(memory_space=pltpu.VMEM)


def smem_spec():
    return pl.BlockSpec(memory_space=pltpu.SMEM)


def any_spec():
    return pl.BlockSpec(memory_space=pl.ANY)


def cost(flops, moved):
    return pl.CostEstimate(flops=int(flops), bytes_accessed=int(moved), transcendentals=0)


def call(kernel, out_shape, inputs, price, scratch=(), limit=16):
    many = isinstance(out_shape, tuple)
    return pl.pallas_call(
        kernel,
        out_shape=out_shape,
        in_specs=[vmem_spec()] * inputs,
        out_specs=(vmem_spec(),) * len(out_shape) if many else vmem_spec(),
        scratch_shapes=list(scratch),
        cost_estimate=price,
        compiler_params=pltpu.CompilerParams(vmem_limit_bytes=limit << 20),
    )


def dot_nt(a, b):
    return lax.dot_general(a, b, (((1,), (1,)), ((), ())), preferred_element_type=f32)


def dot_nn(a, b):
    return lax.dot_general(a, b, (((1,), (0,)), ((), ())), preferred_element_type=f32)


def dot_tn(a, b):
    return lax.dot_general(a, b, (((0,), (0,)), ((), ())), preferred_element_type=f32)


def turn(v, n):
    return pltpu.roll(v, n % 128, v.ndim - 1)


def lanes_of(shape):
    return lax.broadcasted_iota(jnp.int32, shape, len(shape) - 1)


def rounded(v):
    return v.astype(bf16).astype(f32)


def pack_kernel(a_ref, q_ref, k_ref, g_ref, o_ref):
    row = lax.broadcasted_iota(jnp.int32, (384, 512), 0)
    place = (row & 15) * 32 + (row >> 4)
    pick = jnp.where(lanes_of((384, 512)) == place, 1.0, 0.0).astype(bf16)
    lines = dot_nn(a_ref[...], pick)
    lane = lanes_of((16, 128))
    gain = jnp.broadcast_to(g_ref[...], (16, 16))
    diagonal = lax.broadcasted_iota(jnp.int32, (16, 16), 0) == lanes_of((16, 16))
    gain = jnp.sum(jnp.where(diagonal, gain, 0.0), axis=1, keepdims=True)
    query = q_ref[...].astype(f32)
    key = k_ref[...].astype(f32)
    rope = jnp.concatenate([key[:, 256:288], jnp.zeros((16, 96), f32)], axis=1)
    columns = []
    for t in range(8):
        tile = query[:, (t // 2) * 128 : (t // 2) * 128 + 128]
        line = turn(tile, 24 - (t % 2) * 64)
        tile = key[:, (t // 4) * 128 : (t // 4) * 128 + 128]
        line = jnp.where(lane < 88, line, turn(tile, 88 - (t % 4) * 32))
        line = jnp.where(lane < 120, line, turn(rope, 120 - 4 * t))
        columns.append(jnp.where(lane < 124, line, jnp.where(lane == 124, gain, 0.0)))
    for j in range(16):
        tile = lines[:, (j // 4) * 128 : (j // 4) * 128 + 128]
        tile = turn(tile, -(j % 4) * 32) if j % 4 else tile
        for t in range(8):
            o_ref[j * 8 + t] = jnp.where(lane < 24, tile, columns[t]).astype(bf16)


def pack(a, q, k, g):
    return call(
        pack_kernel, jax.ShapeDtypeStruct((128, 16, 128), bf16), 4, cost(1e8, 1e6)
    )(a, q, k, g)


def down_kernel(x_ref, o_ref):
    x = x_ref[...]
    wide = x.astype(f32)
    lane = lanes_of(wide.shape)
    scaled = wide * wide[:, 124:125]
    lhs = jnp.where(lane < 24, scaled, turn(wide, 32)).astype(bf16)
    out = dot_tn(lhs, x)
    cross = out[32:56, :]
    row = lax.broadcasted_iota(jnp.int32, cross.shape, 0)
    squares = jnp.sum(jnp.where(row == lanes_of(cross.shape), cross, 0.0), axis=1, keepdims=True)
    o_ref[...] = jnp.broadcast_to(out[0:24, :] * lax.rsqrt(squares / D + EPS), o_ref.shape)


def down(x):
    return call(
        down_kernel,
        jax.ShapeDtypeStruct((8, 24, 128), f32),
        1,
        cost(2 * 128 * 128 * 2048, x.size * 2),
    )(x)


def query_kernel(t_ref, y_ref, gq_ref, gk_ref, cos_ref, sin_ref, w_ref, o_ref, block):
    mine = t_ref[0]
    lane = lanes_of((24, 128))
    parts = [y_ref[t] for t in range(8)]
    raw = [
        jnp.where(lane < 64, turn(parts[2 * a], -24), turn(parts[2 * a + 1], 40)) for a in range(4)
    ]
    squares = sum(jnp.sum(r * r, axis=1, keepdims=True) for r in raw)
    scale = lax.rsqrt(squares / 512.0 + EPS)
    low = jnp.concatenate(
        [raw[a] * scale * gq_ref[a : a + 1, :] for a in range(4)], axis=1
    ).astype(bf16)
    lats = []
    for half in range(2):
        lat = turn(parts[4 * half], -88)
        for u in range(1, 4):
            lat = jnp.where(lane >= u * 32, turn(parts[4 * half + u], u * 32 - 88), lat)
        lats.append(lat)
    squares = sum(jnp.sum(r * r, axis=1, keepdims=True) for r in lats)
    scale = lax.rsqrt(squares / 256.0 + EPS)
    lats = [rounded(lats[h] * scale * gk_ref[h : h + 1, :]) for h in range(2)]
    turned = turn(parts[0], -120)
    for t in range(1, 8):
        turned = jnp.where(lane >= 4 * t, turn(parts[t], 4 * t - 120), turned)
    cosine, sine = cos_ref[...], sin_ref[...]

    def rotate(v):
        partner = jnp.where(lane < 16, turn(v, -16), turn(v, 16))
        return v * cosine + partner * sine

    def own(tile):
        row = lax.broadcasted_iota(jnp.int32, tile.shape, 0)
        line = jnp.sum(jnp.where(row == mine, tile, 0.0), axis=0, keepdims=True)
        return jnp.broadcast_to(line, tile.shape)

    key_rope = rounded(rotate(turned))
    ropes = []
    query_rope = []
    for hh in range(2):
        lat = dot_nt(low, w_ref[hh, 0:256, :])
        rope = dot_nt(low, w_ref[hh, 256:288, :])
        rope = rotate(jnp.concatenate([rope, jnp.zeros((24, 96), f32)], axis=1))
        query_rope.append(rope)
        for s in range(3):
            for half in range(2):
                block[:, (s * 2 + hh) * 2 + half, :] = lat[
                    s * 8 : s * 8 + 8, half * 128 : half * 128 + 128
                ]
    for s in range(3):
        for half in range(2):
            block[:, 12 + s * 2 + half, :] = own(lats[half][s * 8 : s * 8 + 8, :])
    for s in range(3):
        for hh in range(2):
            ropes.append(query_rope[hh][s * 8 : s * 8 + 8, :])
    for s in range(3):
        ropes.append(own(key_rope[s * 8 : s * 8 + 8, :]))
    small = lanes_of((8, 128))
    for row in range(3):
        line = jnp.zeros((8, 128), f32)
        for n in range(4 * row, min(4 * row + 4, 9)):
            at = (n % 4) * 32
            line = jnp.where((small >= at) & (small < at + 32), turn(ropes[n], at), line)
        block[:, 18 + row, :] = line
        block[:, 21 + row, :] = jnp.zeros((8, 128), f32)
    packed = block[...].astype(bf16)
    for copy in range(16):
        o_ref[copy * 8 : copy * 8 + 8] = packed


def queries(mine, y, gq, gk, cosine, sine, w):
    return pl.pallas_call(
        query_kernel,
        out_shape=jax.ShapeDtypeStruct((128, 24, 128), bf16),
        in_specs=[smem_spec()] + [vmem_spec()] * 6,
        out_specs=vmem_spec(),
        scratch_shapes=[VMEM((8, 24, 128), f32)],
        cost_estimate=cost(2 * 24 * 512 * 576, 128 * 24 * 256),
        compiler_params=pltpu.CompilerParams(vmem_limit_bytes=16 << 20),
        name="queries",
    )(mine, y, gq, gk, cosine, sine, w)


CHUNK = 512


def attend_kernel(
    n_ref, z_ref, cache_ref, anc_ref, wv_ref, o_ref, fresh_ref, keys, wide, lines, part, lam, score, sems
):
    mine = n_ref[24]

    def fetch(s):
        return pltpu.make_async_copy(cache_ref.at[s * 8 + mine], keys.at[s], sems.at[s])

    for s in range(3):
        fetch(s).start()
    wide[...] = z_ref[...].astype(f32)
    lane = lanes_of((128, 128))
    packed = [wide[:, 18 + r, :] for r in range(3)]

    def rope_of(n):
        v = packed[n // 4]
        v = turn(v, -(n % 4) * 32) if n % 4 else v
        return jnp.where(lane < 32, v, 0.0)

    for s in range(3):
        for half in range(2):
            lines[s, half] = wide[:, 12 + s * 2 + half, :]
        lines[s, 2] = rope_of(6 + s)

    def fresh_of(s, t):
        return jnp.concatenate(
            [lines[s, a, pl.ds(t, 16, stride=8), :] for a in range(3)], axis=1
        ).astype(bf16)

    for s in range(3):
        for t in range(8):
            fresh_ref[s * 8 + t] = fresh_of(s, t)
    slot = lanes_of((256, 16))
    for s in range(3):
        off = n_ref[s * 8 + mine]
        fresh = fresh_of(s, mine)
        lat = jnp.concatenate(
            [
                jnp.concatenate(
                    [wide[:, (s * 2 + hh) * 2, :], wide[:, (s * 2 + hh) * 2 + 1, :]], axis=1
                )
                for hh in range(2)
            ],
            axis=0,
        ).astype(bf16)
        rope = jnp.concatenate([rope_of(s * 2 + hh)[:, 0:32] for hh in range(2)], axis=0).astype(
            bf16
        )
        near = (dot_nt(lat, fresh[:, 0:256]) + dot_nt(rope, fresh[:, 256:288])) * SCALE
        anc = anc_ref[s][:, 0:16]
        seen = (
            (jnp.concatenate([anc, anc], axis=0) > 0.5) & (slot + off >= 0) & (slot + off < SPAN)
        )
        near = jnp.where(seen, near, MASKED)
        top = jnp.max(near, axis=1, keepdims=True)
        fetch(s).wait()
        for c in range(SPAN // CHUNK):
            cols = slice(c * CHUNK, (c + 1) * CHUNK)
            got = (
                dot_nn(lat, keys[s, 0:256, cols]) + dot_nn(rope, keys[s, 256:288, cols])
            ) * SCALE
            got = jnp.where(lanes_of(got.shape) + c * CHUNK < off, got, MASKED)
            score[:, cols] = got
            top = jnp.maximum(top, jnp.max(got, axis=1, keepdims=True))
        weight = jnp.where(seen, jnp.exp(near - top), 0.0)
        total = jnp.sum(weight, axis=1, keepdims=True)
        acc = dot_nn(weight.astype(bf16), fresh[:, 0:256])
        for c in range(SPAN // CHUNK):
            cols = slice(c * CHUNK, (c + 1) * CHUNK)
            got = score[:, cols]
            weight = jnp.where(
                lanes_of(got.shape) + c * CHUNK < off, jnp.exp(got - top), 0.0
            )
            total = total + jnp.sum(weight, axis=1, keepdims=True)
            acc = acc + dot_nt(weight.astype(bf16), keys[s, 0:256, cols])
        acc = rounded(acc / jnp.maximum(total, 1.0))
        for half in range(2):
            part[s, half] = acc[:, half * 128 : half * 128 + 128]
        level = jnp.where(total > 0.0, top + jnp.log(jnp.maximum(total, 1.0)), MASKED)
        lam[s] = jnp.broadcast_to(level, (256, 128))
    small = lanes_of((8, 128))
    for h in range(16):
        pieces = []
        level = jnp.zeros((8, 128), f32)
        for half in range(2):
            for s in range(3):
                rows = pl.ds((h % 2) * 128 + half * 64 + h // 2, 8, stride=8)
                pieces.append(jnp.concatenate([part[s, a, rows, :] for a in range(2)], axis=1))
                level = jnp.where(small // 4 == half * 3 + s, lam[s, rows, :], level)
        out = dot_nt(jnp.concatenate(pieces, axis=0).astype(bf16), wv_ref[h])
        out = jnp.concatenate([out[0:24], out[24:48]], axis=1)
        first = rounded(level)
        second = rounded(level - first)
        third = (level - first) - second
        level = jnp.where(small % 4 == 0, first, jnp.where(small % 4 == 1, second, third))
        level = jnp.where(small % 4 == 3, 0.0, level)
        o_ref[h] = jnp.concatenate([out, level], axis=0).astype(bf16)


def attend(numbers, z, cache, anc, wv):
    return pl.pallas_call(
        attend_kernel,
        out_shape=(
            jax.ShapeDtypeStruct((16, 32, 128), bf16),
            jax.ShapeDtypeStruct((24, 16, 384), bf16),
        ),
        in_specs=[smem_spec(), vmem_spec(), any_spec(), vmem_spec(), vmem_spec()],
        out_specs=(vmem_spec(), vmem_spec()),
        scratch_shapes=[
            VMEM((3, LINES, SPAN), bf16),
            VMEM((128, 24, 128), f32),
            VMEM((3, 3, 128, 128), f32),
            VMEM((3, 2, 256, 128), f32),
            VMEM((3, 256, 128), f32),
            VMEM((256, SPAN), f32),
            pltpu.SemaphoreType.DMA((3,)),
        ],
        cost_estimate=cost(3 * 2 * 256 * 2048 * 544, 3 * LINES * SPAN * 2),
        compiler_params=pltpu.CompilerParams(vmem_limit_bytes=40 << 20),
        name="attend",
    )(numbers, z, cache, anc, wv)


def combine_kernel(v_ref, o_ref):
    v = v_ref[...].astype(f32)
    level = v[:, 24:32, :]
    level = (level + turn(level, -1)) + turn(level, -2)
    lane = lanes_of((16, 8, 128))
    outs = []
    for s in range(3):
        low, high = (level[:, :, 4 * (h * 3 + s) : 4 * (h * 3 + s) + 1] for h in range(2))
        both = jnp.where(lane < 64, low, high)
        share = jnp.exp(both - jnp.max(both, axis=0, keepdims=True))
        summed = jnp.sum(share * v[:, s * 8 : s * 8 + 8, :], axis=0)
        outs.append(summed / jnp.sum(share, axis=0))
    o_ref[...] = jnp.broadcast_to(jnp.concatenate(outs, axis=0).astype(bf16), o_ref.shape)


def combine(v):
    return call(combine_kernel, jax.ShapeDtypeStruct((16, 24, 128), bf16), 1, cost(1e6, 1e5))(v)


def mix_kernel(t_ref, u_ref, *refs):
    w_refs, (o_ref, s_ref) = refs[:8], refs[8:]
    lane = lanes_of((24, 128))
    mixed = jnp.zeros((48, 128), f32)
    for k in range(8):
        p = (t_ref[0] - k) & 7
        a, b = u_ref[2 * p].astype(f32), u_ref[2 * p + 1].astype(f32)
        left = jnp.where(lane < 64, a, turn(b, 64))
        right = jnp.where(lane < 64, turn(a, 64), b)
        lhs = jnp.concatenate([left, right], axis=0).astype(bf16)
        mixed = mixed + dot_nn(lhs, w_refs[k][...])
    o_ref[...] = mixed
    squares = jnp.broadcast_to(jnp.sum(mixed * mixed, axis=1, keepdims=True), mixed.shape)
    row = lax.broadcasted_iota(jnp.int32, (48, 128), 0)
    line = jnp.sum(jnp.where(row == lanes_of((48, 128)), squares, 0.0), axis=0, keepdims=True)
    s_ref[...] = jnp.broadcast_to(line[None], s_ref.shape)


def mix(t, u, w):
    return pl.pallas_call(
        mix_kernel,
        out_shape=(
            jax.ShapeDtypeStruct((48, 128), f32),
            jax.ShapeDtypeStruct((16, 8, 128), f32),
        ),
        in_specs=[smem_spec()] + [vmem_spec()] * 9,
        out_specs=(vmem_spec(),) * 2,
        cost_estimate=cost(2 * 48 * 1024 * 128, 4e5),
        compiler_params=pltpu.CompilerParams(vmem_limit_bytes=16 << 20),
        name="mix",
    )(t, u, *w)


def finish_kernel(m_ref, s_ref, g_ref, o_ref):
    total = jnp.sum(s_ref[...], axis=0)[0:1]
    inverse = lax.rsqrt(total / D + EPS)
    row = lax.broadcasted_iota(jnp.int32, (48, 128), 0)
    same = row == lanes_of((48, 128))
    column = jnp.sum(jnp.where(same, inverse, 0.0), axis=1, keepdims=True)
    out = m_ref[...] * column * g_ref[...]
    rows = []
    for s in range(3):
        rows += [out[s * 8 : s * 8 + 8], out[24 + s * 8 : 32 + s * 8]]
    rows = jnp.concatenate(rows, axis=0).astype(bf16)
    o_ref[...] = jnp.broadcast_to(rows, o_ref.shape)


def finish(m, s, g):
    return call(finish_kernel, jax.ShapeDtypeStruct((8, 48, 128), bf16), 3, cost(1e6, 4e5))(m, s, g)


def spread_kernel(m_ref, o_ref):
    for t in range(8):
        for s in range(3):
            o_ref[(s * 8 + t) * 16 : (s * 8 + t) * 16 + 16, :] = m_ref[t, s * 16 : s * 16 + 16]


def spread(m):
    return call(spread_kernel, jax.ShapeDtypeStruct((384, 128), bf16), 1, cost(1e6, 4e5))(m)


DEPTH = 4


def copy_rows(source, target, buffer, into, outof, start, stop):
    count = stop - start

    def read(n, b):
        return pltpu.make_async_copy(source.at[start + n], buffer.at[b], into.at[b])

    def write(n, b):
        return pltpu.make_async_copy(buffer.at[b], target.at[start + n], outof.at[b])

    for n in range(min(DEPTH, count)):
        read(n, n).start()

    def body(n, carry):
        b = lax.rem(n, 2 * DEPTH)
        read(n, b).wait()
        write(n, b).start()

        @pl.when(n + DEPTH < count)
        def _():
            later = lax.rem(n + DEPTH, 2 * DEPTH)

            @pl.when(n >= DEPTH)
            def _():
                write(n - DEPTH, later).wait()

            read(n + DEPTH, later).start()

        return carry

    lax.fori_loop(0, count, body, 0)

    def drain(n, carry):
        write(n, lax.rem(n, 2 * DEPTH)).wait()
        return carry

    lax.fori_loop(max(0, count - 2 * DEPTH), count, drain, 0)


def copy_cache(cache, so_far, start, stop):
    def kernel(*refs):
        source = refs[0]
        target, buffer, into, outof = refs[-4:]
        copy_rows(source, target, buffer, into, outof, start, stop)

    first = so_far is None
    return pl.pallas_call(
        kernel,
        out_shape=jax.ShapeDtypeStruct(cache.shape, cache.dtype),
        in_specs=[any_spec()] * (1 if first else 2),
        out_specs=any_spec(),
        scratch_shapes=[
            VMEM((2 * DEPTH, LINES, SPAN), bf16),
            pltpu.SemaphoreType.DMA((2 * DEPTH,)),
            pltpu.SemaphoreType.DMA((2 * DEPTH,)),
        ],
        input_output_aliases={} if first else {1: 0},
        cost_estimate=cost((stop - start) * 9e8, (stop - start) * LINES * SPAN * 4),
        compiler_params=pltpu.CompilerParams(vmem_limit_bytes=40 << 20),
        name="copy_cache",
    )(*((cache,) if first else (cache, so_far)))


WINDOW = 256


def place_kernel(n_ref, cache_ref, fresh_ref, old_ref, o_ref, buffer, into, outof):
    def where_is(s):
        off = n_ref[s]
        hit = (off > -PROPS) & (off < SPAN)
        first = jnp.clip(off, 0, SPAN - 1)
        first = jnp.minimum((first // 128) * 128, SPAN - WINDOW)
        return off, hit, pl.multiple_of(first, 128)

    def read(s, first):
        return pltpu.make_async_copy(
            cache_ref.at[s, :, pl.ds(first, WINDOW)], buffer.at[s], into.at[s]
        )

    def write(s, first):
        return pltpu.make_async_copy(
            buffer.at[s], o_ref.at[s, :, pl.ds(first, WINDOW)], outof.at[s]
        )

    def begin(s, carry):
        _, hit, first = where_is(s)

        @pl.when(hit)
        def _():
            read(s, first).start()

        return carry

    def change(s, carry):
        off, hit, first = where_is(s)

        @pl.when(hit)
        def _():
            read(s, first).wait()
            at = lanes_of((PROPS, WINDOW)) + (first - off)
            pick = at == lax.broadcasted_iota(jnp.int32, (PROPS, WINDOW), 0)
            new = dot_tn(fresh_ref[s], jnp.where(pick, 1.0, 0.0).astype(bf16))[0:LINES]
            line = lanes_of((LINES, WINDOW)) + (first - off)
            old = buffer[s].astype(f32)
            buffer[s] = jnp.where((line >= 0) & (line < PROPS), new, old).astype(bf16)
            write(s, first).start()

        return carry

    def end(s, carry):
        _, hit, first = where_is(s)

        @pl.when(hit)
        def _():
            write(s, first).wait()

        return carry

    lax.fori_loop(0, SEQS, begin, 0)
    lax.fori_loop(0, SEQS, change, 0)
    lax.fori_loop(0, SEQS, end, 0)


def place(numbers, cache, fresh, so_far):
    return pl.pallas_call(
        place_kernel,
        out_shape=jax.ShapeDtypeStruct(cache.shape, cache.dtype),
        in_specs=[smem_spec(), any_spec(), vmem_spec(), any_spec()],
        out_specs=any_spec(),
        scratch_shapes=[
            VMEM((SEQS, LINES, WINDOW), bf16),
            pltpu.SemaphoreType.DMA((SEQS,)),
            pltpu.SemaphoreType.DMA((SEQS,)),
        ],
        input_output_aliases={3: 0},
        cost_estimate=cost(1e9, 2e6),
        compiler_params=pltpu.CompilerParams(vmem_limit_bytes=40 << 20),
        name="place",
    )(numbers, cache, fresh, so_far)


def ancestry(parents):
    _, prop_count = parents.shape
    slot_ids = jnp.arange(prop_count, dtype=jnp.int32)
    parent_links = (parents[:, :, None] == slot_ids[None, None, :]).astype(f32)
    identity = jnp.broadcast_to(jnp.eye(prop_count, dtype=f32), parent_links.shape)
    reached = jnp.minimum(identity + parent_links, 1.0)
    for _ in range((prop_count - 1).bit_length()):
        reached = jnp.minimum(
            jnp.einsum("sij,sjk->sik", reached, reached, precision=lax.Precision.HIGHEST), 1.0
        )
    depths = (jnp.sum(reached, axis=-1) - 1.0).astype(jnp.int32)
    return (reached, depths)


def exchange(value, axis):
    return lax.all_to_all(value, axis, 0, 0, tiled=True)


def layer(
    activations,
    latent_cache,
    lengths,
    accepted,
    parents,
    w_query_down,
    w_key_down,
    gain_input,
    gain_query,
    gain_key,
    w_query,
    w_value,
    w_out,
    gain_output,
):
    j = lax.axis_index("kv")
    t = lax.axis_index("tp")
    mine = t[None].astype(jnp.int32)
    cache = jnp.transpose(latent_cache, (0, 2, 1))

    x = pack(jnp.transpose(activations), w_query_down, w_key_down, gain_input.astype(f32)[None])
    x = exchange(x, ALL).reshape(2048, 128)
    y = exchange(down(x), "tp")

    reached, depths = ancestry(parents)
    filled = lengths + accepted
    my_depths = lax.dynamic_slice_in_dim(depths, j, 1, 1)[:, 0]
    half = ROPE_DIM // 2
    frequency = ROPE_BASE ** (-jnp.arange(half, dtype=f32) / half)
    angles = (filled + my_depths).astype(f32)[:, None] * frequency[None, :]
    cosine, sine = jnp.cos(angles), jnp.sin(angles)
    nothing = jnp.zeros((SEQS, 96), f32)
    cosine = jnp.concatenate([cosine, cosine, nothing], axis=1)
    sine = jnp.concatenate([-sine, sine, nothing], axis=1)
    numbers = jnp.concatenate([filled - j * SPAN, t[None]]).astype(jnp.int32)
    group = lax.dynamic_index_in_dim(reached.reshape(3, 8, PROPS, PROPS), t, 1, False)
    anc = jnp.repeat(jnp.pad(group, ((0, 0), (0, 0), (0, 112))), 8, axis=1)

    wq = jnp.transpose(w_query, (1, 2, 0))
    wv = jnp.transpose(w_value, (0, 2, 1))
    z = queries(
        mine,
        y,
        gain_query.astype(f32).reshape(4, 128),
        gain_key.astype(f32).reshape(2, 128),
        cosine,
        sine,
        wq,
    )
    z = exchange(z, ALL)
    sent, fresh = attend(numbers, z, cache, anc, wv)

    updated = None
    for n in range(len(CUTS) - 1):
        updated = copy_cache(cache, updated, CUTS[n], CUTS[n + 1])
    updated = place(numbers, cache, fresh, updated)

    w_here = [w_out]
    for k in range(1, 8):
        w_here.append(lax.ppermute(w_out, "tp", [(n, (n + k) % 8) for n in range(8)]))
    attended = combine(exchange(sent, "kv"))
    mixed, squares = mix(mine, exchange(attended, "kv"), w_here)
    squares = exchange(squares, "kv")
    result = finish(mixed, squares, gain_output.astype(f32)[None])
    result = spread(exchange(result, "tp"))
    return (result, jnp.transpose(updated, (0, 2, 1)))


CUTS = (0, 5, 9, 20, 24)


def solution(mesh):
    return jax.shard_map(
        layer,
        mesh=mesh,
        in_specs=(
            P(None, ALL),
            P(None, "kv", None),
            P(),
            P(),
            P(),
            P(ALL, None),
            P(ALL, None),
            P(ALL),
            P(),
            P(),
            P(None, "tp", None),
            P(),
            P("tp", "kv"),
            P("kv"),
        ),
        out_specs=(P(None, "kv"), P(None, "kv", None)),
        check_vma=False,
    )
```

```python
import jax
import jax.numpy as jnp
from jax import lax
from jax.experimental import pallas as pl
from jax.experimental.pallas import tpu as pltpu
from jax.sharding import PartitionSpec as P


f32 = jnp.float32
bf16 = jnp.bfloat16

D = 2048
SEQS = 24
PROPS = 16
SPAN = 2048
KV_RANK = 256
ROPE_DIM = 32
LINES = 288
SCALE = 96.0 ** (-0.5)
EPS = 1e-06
ROPE_BASE = 10000.0
MASKED = -1e30
ALL = ("kv", "tp")
VMEM = pltpu.VMEM


def vmem_spec():
    return pl.BlockSpec(memory_space=pltpu.VMEM)


def smem_spec():
    return pl.BlockSpec(memory_space=pltpu.SMEM)


def any_spec():
    return pl.BlockSpec(memory_space=pl.ANY)


def cost(flops, moved):
    return pl.CostEstimate(flops=int(flops), bytes_accessed=int(moved), transcendentals=0)


def call(kernel, out_shape, inputs, price, scratch=(), limit=16):
    many = isinstance(out_shape, tuple)
    return pl.pallas_call(
        kernel,
        out_shape=out_shape,
        in_specs=[vmem_spec()] * inputs,
        out_specs=(vmem_spec(),) * len(out_shape) if many else vmem_spec(),
        scratch_shapes=list(scratch),
        cost_estimate=price,
        compiler_params=pltpu.CompilerParams(vmem_limit_bytes=limit << 20),
    )


def dot_nt(a, b):
    return lax.dot_general(a, b, (((1,), (1,)), ((), ())), preferred_element_type=f32)


def dot_nn(a, b):
    return lax.dot_general(a, b, (((1,), (0,)), ((), ())), preferred_element_type=f32)


def dot_tn(a, b):
    return lax.dot_general(a, b, (((0,), (0,)), ((), ())), preferred_element_type=f32)


def turn(v, n):
    return pltpu.roll(v, n % 128, v.ndim - 1)


def lanes_of(shape):
    return lax.broadcasted_iota(jnp.int32, shape, len(shape) - 1)


def rounded(v):
    return v.astype(bf16).astype(f32)


def pack_kernel(a_ref, q_ref, k_ref, g_ref, o_ref):
    row = lax.broadcasted_iota(jnp.int32, (384, 512), 0)
    place = (row & 15) * 32 + (row >> 4)
    pick = jnp.where(lanes_of((384, 512)) == place, 1.0, 0.0).astype(bf16)
    lines = dot_nn(a_ref[...], pick)
    lane = lanes_of((16, 128))
    gain = jnp.broadcast_to(g_ref[...].astype(f32), (16, 16))
    diagonal = lax.broadcasted_iota(jnp.int32, (16, 16), 0) == lanes_of((16, 16))
    gain = jnp.sum(jnp.where(diagonal, gain, 0.0), axis=1, keepdims=True)
    query = q_ref[...].astype(f32)
    key = k_ref[...].astype(f32)
    rope = jnp.concatenate([key[:, 256:288], jnp.zeros((16, 96), f32)], axis=1)
    columns = []
    for t in range(8):
        tile = query[:, (t // 2) * 128 : (t // 2) * 128 + 128]
        line = turn(tile, 24 - (t % 2) * 64)
        tile = key[:, (t // 4) * 128 : (t // 4) * 128 + 128]
        line = jnp.where(lane < 88, line, turn(tile, 88 - (t % 4) * 32))
        line = jnp.where(lane < 120, line, turn(rope, 120 - 4 * t))
        columns.append(jnp.where(lane < 124, line, jnp.where(lane == 124, gain, 0.0)))
    for j in range(16):
        tile = lines[:, (j // 4) * 128 : (j // 4) * 128 + 128]
        tile = turn(tile, -(j % 4) * 32) if j % 4 else tile
        for t in range(8):
            o_ref[j * 8 + t] = jnp.where(lane < 24, tile, columns[t]).astype(bf16)


def pack(a, q, k, g):
    return call(
        pack_kernel, jax.ShapeDtypeStruct((128, 16, 128), bf16), 4, cost(1e8, 1e6), limit=60
    )(a, q, k, g)


def down_kernel(x_ref, o_ref):
    x = x_ref[...]
    wide = x.astype(f32)
    lane = lanes_of(wide.shape)
    scaled = wide * wide[:, 124:125]
    lhs = jnp.where(lane < 24, scaled, turn(wide, 32)).astype(bf16)
    out = dot_tn(lhs, x)
    cross = out[32:56, :]
    row = lax.broadcasted_iota(jnp.int32, cross.shape, 0)
    squares = jnp.sum(jnp.where(row == lanes_of(cross.shape), cross, 0.0), axis=1, keepdims=True)
    o_ref[...] = jnp.broadcast_to(out[0:24, :] * lax.rsqrt(squares / D + EPS), o_ref.shape)


def down(x):
    return call(
        down_kernel,
        jax.ShapeDtypeStruct((8, 24, 128), f32),
        1,
        cost(2 * 128 * 128 * 2048, x.size * 2),
    )(x)


def query_kernel(t_ref, y_ref, gq_ref, gk_ref, cos_ref, sin_ref, w_ref, o_ref, block):
    mine = t_ref[0]
    lane = lanes_of((24, 128))
    parts = [y_ref[t] for t in range(8)]
    raw = [
        jnp.where(lane < 64, turn(parts[2 * a], -24), turn(parts[2 * a + 1], 40)) for a in range(4)
    ]
    squares = sum(jnp.sum(r * r, axis=1, keepdims=True) for r in raw)
    scale = lax.rsqrt(squares / 512.0 + EPS)
    low = jnp.concatenate(
        [raw[a] * scale * gq_ref[a : a + 1, :] for a in range(4)], axis=1
    ).astype(bf16)
    lats = []
    for half in range(2):
        lat = turn(parts[4 * half], -88)
        for u in range(1, 4):
            lat = jnp.where(lane >= u * 32, turn(parts[4 * half + u], u * 32 - 88), lat)
        lats.append(lat)
    squares = sum(jnp.sum(r * r, axis=1, keepdims=True) for r in lats)
    scale = lax.rsqrt(squares / 256.0 + EPS)
    lats = [rounded(lats[h] * scale * gk_ref[h : h + 1, :]) for h in range(2)]
    turned = turn(parts[0], -120)
    for t in range(1, 8):
        turned = jnp.where(lane >= 4 * t, turn(parts[t], 4 * t - 120), turned)
    cosine, sine = cos_ref[...], sin_ref[...]

    def rotate(v):
        partner = jnp.where(lane < 16, turn(v, -16), turn(v, 16))
        return v * cosine + partner * sine

    def own(tile):
        row = lax.broadcasted_iota(jnp.int32, tile.shape, 0)
        line = jnp.sum(jnp.where(row == mine, tile, 0.0), axis=0, keepdims=True)
        return jnp.broadcast_to(line, tile.shape)

    key_rope = rounded(rotate(turned))
    ropes = []
    query_rope = []
    for hh in range(2):
        lat = dot_nt(low, w_ref[hh, 0:256, :])
        rope = dot_nt(low, w_ref[hh, 256:288, :])
        rope = rotate(jnp.concatenate([rope, jnp.zeros((24, 96), f32)], axis=1))
        query_rope.append(rope)
        for s in range(3):
            for half in range(2):
                block[:, (s * 2 + hh) * 2 + half, :] = lat[
                    s * 8 : s * 8 + 8, half * 128 : half * 128 + 128
                ]
    for s in range(3):
        for half in range(2):
            block[:, 12 + s * 2 + half, :] = own(lats[half][s * 8 : s * 8 + 8, :])
    for s in range(3):
        for hh in range(2):
            ropes.append(query_rope[hh][s * 8 : s * 8 + 8, :])
    for s in range(3):
        ropes.append(own(key_rope[s * 8 : s * 8 + 8, :]))
    small = lanes_of((8, 128))
    for row in range(3):
        line = jnp.zeros((8, 128), f32)
        for n in range(4 * row, min(4 * row + 4, 9)):
            at = (n % 4) * 32
            line = jnp.where((small >= at) & (small < at + 32), turn(ropes[n], at), line)
        block[:, 18 + row, :] = line
        block[:, 21 + row, :] = jnp.zeros((8, 128), f32)
    packed = block[...].astype(bf16)
    for copy in range(16):
        o_ref[copy * 8 : copy * 8 + 8] = packed


def queries(mine, y, gq, gk, cosine, sine, w):
    return pl.pallas_call(
        query_kernel,
        out_shape=jax.ShapeDtypeStruct((128, 24, 128), bf16),
        in_specs=[smem_spec()] + [vmem_spec()] * 6,
        out_specs=vmem_spec(),
        scratch_shapes=[VMEM((8, 24, 128), f32)],
        cost_estimate=cost(2 * 24 * 512 * 576, 128 * 24 * 256),
        compiler_params=pltpu.CompilerParams(vmem_limit_bytes=16 << 20),
        name="queries",
    )(mine, y, gq, gk, cosine, sine, w)


CHUNK = 512
LOG2E = 1.4426950408889634


def attend_kernel(
    n_ref,
    z_ref,
    cache_ref,
    anc_ref,
    wv_ref,
    o_ref,
    fresh_ref,
    keys,
    wide,
    lines,
    part,
    lam,
    score,
    prob,
    sems,
):
    mine = n_ref[24]

    def fetch(s):
        return pltpu.make_async_copy(cache_ref.at[s * 8 + mine], keys.at[s], sems.at[s])

    for s in range(3):
        fetch(s).start()
    wide[...] = z_ref[...].astype(f32)
    lane = lanes_of((128, 128))
    packed = [wide[:, 18 + r, :] for r in range(3)]

    def rope_of(n):
        v = packed[n // 4]
        v = turn(v, -(n % 4) * 32) if n % 4 else v
        return jnp.where(lane < 32, v, 0.0)

    for s in range(3):
        for half in range(2):
            lines[s, half] = wide[:, 12 + s * 2 + half, :]
        lines[s, 2] = rope_of(6 + s)

    def fresh_of(s, t):
        return jnp.concatenate(
            [lines[s, a, pl.ds(t, 16, stride=8), :] for a in range(3)], axis=1
        ).astype(bf16)

    for s in range(3):
        for t in range(8):
            fresh_ref[s * 8 + t] = fresh_of(s, t)
    slot = lanes_of((256, 16))

    def tiles(v, join):
        out = v[:, 0:128]
        for n in range(1, v.shape[1] // 128):
            out = join(out, v[:, n * 128 : n * 128 + 128])
        return out

    def scores(s):
        off = n_ref[s * 8 + mine]
        fresh = fresh_of(s, mine)[:, 0:LINES]
        query = jnp.concatenate(
            [
                jnp.concatenate(
                    [
                        wide[:, (s * 2 + hh) * 2, :],
                        wide[:, (s * 2 + hh) * 2 + 1, :],
                        rope_of(s * 2 + hh)[:, 0:ROPE_DIM],
                    ],
                    axis=1,
                )
                for hh in range(2)
            ],
            axis=0,
        ).astype(bf16)
        near = dot_nt(query, fresh) * (SCALE * LOG2E)
        anc = anc_ref[s][:, 0:16]
        seen = (
            (jnp.concatenate([anc, anc], axis=0) > 0.5) & (slot + off >= 0) & (slot + off < SPAN)
        )
        near = jnp.where(seen, near, MASKED)
        most = None
        for c in range(SPAN // CHUNK):
            cols = slice(c * CHUNK, (c + 1) * CHUNK)
            bias = jnp.where(lanes_of((1, CHUNK)) + c * CHUNK < off, 0.0, MASKED)
            got = dot_nn(query, keys[s, :, cols]) * (SCALE * LOG2E) + bias
            score[s, :, cols] = got
            got = tiles(got, jnp.maximum)
            most = got if most is None else jnp.maximum(most, got)
        top = jnp.maximum(
            jnp.max(most, axis=1, keepdims=True), jnp.max(near, axis=1, keepdims=True)
        )
        return fresh, near, top

    def values(s, fresh, near, top):
        base = jnp.where(top < 0.1 * MASKED, 0.0, top)
        weight = jnp.exp2(near - base)
        total = jnp.sum(weight, axis=1, keepdims=True)
        acc = dot_nn(weight.astype(bf16), fresh[:, 0:KV_RANK])
        count = None
        for c in range(SPAN // CHUNK):
            cols = slice(c * CHUNK, (c + 1) * CHUNK)
            weight = jnp.exp2(score[s, :, cols] - base)
            prob[s, :, cols] = weight.astype(bf16)
            weight = tiles(weight, jnp.add)
            count = weight if count is None else count + weight
        total = total + jnp.sum(count, axis=1, keepdims=True)
        acc = acc + dot_nt(prob[s], keys[s, 0:KV_RANK, :])
        acc = rounded(acc / jnp.maximum(total, 1.0))
        for half in range(2):
            part[s, half] = acc[:, half * 128 : half * 128 + 128]
        level = jnp.where(total > 0.0, top + jnp.log2(jnp.maximum(total, 1.0)), MASKED)
        lam[s] = jnp.broadcast_to(level, (256, 128))

    fetch(0).wait()
    first = scores(0)
    fetch(1).wait()
    fetch(2).wait()
    second = scores(1)
    values(0, *first)
    third = scores(2)
    values(1, *second)
    values(2, *third)
    small = lanes_of((8, 128))
    for h in range(16):
        pieces = []
        level = jnp.zeros((8, 128), f32)
        for half in range(2):
            for s in range(3):
                rows = pl.ds((h % 2) * 128 + half * 64 + h // 2, 8, stride=8)
                pieces.append(jnp.concatenate([part[s, a, rows, :] for a in range(2)], axis=1))
                level = jnp.where(small // 4 == half * 3 + s, lam[s, rows, :], level)
        out = dot_nt(jnp.concatenate(pieces, axis=0).astype(bf16), wv_ref[h])
        out = jnp.concatenate([out[0:24], out[24:48]], axis=1)
        first = rounded(level)
        second = rounded(level - first)
        third = (level - first) - second
        level = jnp.where(small % 4 == 0, first, jnp.where(small % 4 == 1, second, third))
        level = jnp.where(small % 4 == 3, 0.0, level)
        o_ref[h] = jnp.concatenate([out, level], axis=0).astype(bf16)


def attend(numbers, z, cache, anc, wv):
    return pl.pallas_call(
        attend_kernel,
        out_shape=(
            jax.ShapeDtypeStruct((16, 32, 128), bf16),
            jax.ShapeDtypeStruct((24, 16, 384), bf16),
        ),
        in_specs=[smem_spec(), vmem_spec(), any_spec(), vmem_spec(), vmem_spec()],
        out_specs=(vmem_spec(), vmem_spec()),
        scratch_shapes=[
            VMEM((3, LINES, SPAN), bf16),
            VMEM((128, 24, 128), f32),
            VMEM((3, 3, 128, 128), f32),
            VMEM((3, 2, 256, 128), f32),
            VMEM((3, 256, 128), f32),
            VMEM((3, 256, SPAN), f32),
            VMEM((3, 256, SPAN), bf16),
            pltpu.SemaphoreType.DMA((3,)),
        ],
        cost_estimate=cost(3 * 2 * 256 * 2048 * 544, 3 * LINES * SPAN * 2),
        compiler_params=pltpu.CompilerParams(vmem_limit_bytes=52 << 20),
        name="attend",
    )(numbers, z, cache, anc, wv)


def combine_kernel(v_ref, o_ref):
    v = v_ref[...].astype(f32)
    level = v[:, 24:32, :]
    level = (level + turn(level, -1)) + turn(level, -2)
    lane = lanes_of((16, 8, 128))
    outs = []
    for s in range(3):
        low, high = (level[:, :, 4 * (h * 3 + s) : 4 * (h * 3 + s) + 1] for h in range(2))
        both = jnp.where(lane < 64, low, high)
        share = jnp.exp2(both - jnp.max(both, axis=0, keepdims=True))
        summed = jnp.sum(share * v[:, s * 8 : s * 8 + 8, :], axis=0)
        outs.append(summed / jnp.sum(share, axis=0))
    o_ref[...] = jnp.broadcast_to(jnp.concatenate(outs, axis=0).astype(bf16), o_ref.shape)


def combine(v):
    return call(combine_kernel, jax.ShapeDtypeStruct((16, 24, 128), bf16), 1, cost(1e6, 1e5))(v)


def mix_kernel(t_ref, u_ref, *refs):
    w_refs, (o_ref, s_ref) = refs[:4], refs[4:]
    lane = lanes_of((24, 128))
    mixed = jnp.zeros((48, 128), f32)
    for k in range(4):
        for b in range(2):
            p = ((t_ref[0] - 2 * k) & 7) ^ b
            first, second = u_ref[2 * p].astype(f32), u_ref[2 * p + 1].astype(f32)
            left = jnp.where(lane < 64, first, turn(second, 64))
            right = jnp.where(lane < 64, turn(first, 64), second)
            lhs = jnp.concatenate([left, right], axis=0).astype(bf16)
            mixed = mixed + dot_nn(lhs, w_refs[k][b])
    o_ref[...] = mixed
    squares = jnp.broadcast_to(jnp.sum(mixed * mixed, axis=1, keepdims=True), mixed.shape)
    row = lax.broadcasted_iota(jnp.int32, (48, 128), 0)
    line = jnp.sum(jnp.where(row == lanes_of((48, 128)), squares, 0.0), axis=0, keepdims=True)
    s_ref[...] = jnp.broadcast_to(line[None], s_ref.shape)


def mix(t, u, w):
    return pl.pallas_call(
        mix_kernel,
        out_shape=(
            jax.ShapeDtypeStruct((48, 128), f32),
            jax.ShapeDtypeStruct((128, 1, 128), f32),
        ),
        in_specs=[smem_spec()] + [vmem_spec()] * 5,
        out_specs=(vmem_spec(),) * 2,
        cost_estimate=cost(2 * 48 * 1024 * 128, 4e5),
        compiler_params=pltpu.CompilerParams(vmem_limit_bytes=16 << 20),
        name="mix",
    )(t, u, *w)


def finish_kernel(t_ref, s_ref, g_ref, *refs):
    m_refs, (o_ref, scale) = refs[:8], refs[8:]
    scale[...] = lax.rsqrt(jnp.sum(s_ref[...], axis=0) / D + EPS)
    row = lax.broadcasted_iota(jnp.int32, (48, 128), 0)
    same = row == lanes_of((48, 128))
    gain = g_ref[...]
    for k in range(8):
        p = (t_ref[0] - k) & 7
        inverse = scale[pl.ds(p, 1), :]
        column = jnp.sum(jnp.where(same, inverse, 0.0), axis=1, keepdims=True)
        out = m_refs[k][...] * column * gain
        for s in range(3):
            rows = jnp.concatenate([out[s * 8 : s * 8 + 8], out[24 + s * 8 : 32 + s * 8]], axis=0)
            at = pl.multiple_of((s * 8 + p) * 16, 16)
            o_ref[pl.ds(at, 16), :] = rows.astype(bf16)


def finish(t, s, g, m):
    return pl.pallas_call(
        finish_kernel,
        out_shape=jax.ShapeDtypeStruct((384, 128), bf16),
        in_specs=[smem_spec()] + [vmem_spec()] * 10,
        out_specs=vmem_spec(),
        scratch_shapes=[VMEM((8, 128), f32)],
        cost_estimate=cost(1e6, 4e5),
        compiler_params=pltpu.CompilerParams(vmem_limit_bytes=16 << 20),
        name="finish",
    )(t, s, g, *m)


DEPTH = 4


def copy_rows(source, target, buffer, into, outof, start, stop):
    count = stop - start

    def read(n, b):
        return pltpu.make_async_copy(source.at[start + n], buffer.at[b], into.at[b])

    def write(n, b):
        return pltpu.make_async_copy(buffer.at[b], target.at[start + n], outof.at[b])

    for n in range(min(DEPTH, count)):
        read(n, n).start()

    def body(n, carry):
        b = lax.rem(n, 2 * DEPTH)
        read(n, b).wait()
        write(n, b).start()

        @pl.when(n + DEPTH < count)
        def _():
            later = lax.rem(n + DEPTH, 2 * DEPTH)

            @pl.when(n >= DEPTH)
            def _():
                write(n - DEPTH, later).wait()

            read(n + DEPTH, later).start()

        return carry

    lax.fori_loop(0, count, body, 0)

    def drain(n, carry):
        write(n, lax.rem(n, 2 * DEPTH)).wait()
        return carry

    lax.fori_loop(max(0, count - 2 * DEPTH), count, drain, 0)


def copy_cache(cache, so_far, start, stop):
    def kernel(*refs):
        source = refs[0]
        target, buffer, into, outof = refs[-4:]
        copy_rows(source, target, buffer, into, outof, start, stop)

    first = so_far is None
    return pl.pallas_call(
        kernel,
        out_shape=jax.ShapeDtypeStruct(cache.shape, cache.dtype),
        in_specs=[any_spec()] * (1 if first else 2),
        out_specs=any_spec(),
        scratch_shapes=[
            VMEM((2 * DEPTH, LINES, SPAN), bf16),
            pltpu.SemaphoreType.DMA((2 * DEPTH,)),
            pltpu.SemaphoreType.DMA((2 * DEPTH,)),
        ],
        input_output_aliases={} if first else {1: 0},
        cost_estimate=cost((stop - start) * 9e8, (stop - start) * LINES * SPAN * 4),
        compiler_params=pltpu.CompilerParams(vmem_limit_bytes=40 << 20),
        name="copy_cache",
    )(*((cache,) if first else (cache, so_far)))


WINDOW = 256


def place_kernel(n_ref, cache_ref, fresh_ref, old_ref, o_ref, buffer, into, outof):
    def where_is(s):
        off = n_ref[s]
        hit = (off > -PROPS) & (off < SPAN)
        first = jnp.clip(off, 0, SPAN - 1)
        first = jnp.minimum((first // 128) * 128, SPAN - WINDOW)
        return off, hit, pl.multiple_of(first, 128)

    def read(s, first):
        return pltpu.make_async_copy(
            cache_ref.at[s, :, pl.ds(first, WINDOW)], buffer.at[s], into.at[s]
        )

    def write(s, first):
        return pltpu.make_async_copy(
            buffer.at[s], o_ref.at[s, :, pl.ds(first, WINDOW)], outof.at[s]
        )

    def begin(s, carry):
        _, hit, first = where_is(s)

        @pl.when(hit)
        def _():
            read(s, first).start()

        return carry

    def change(s, carry):
        off, hit, first = where_is(s)

        @pl.when(hit)
        def _():
            read(s, first).wait()
            at = lanes_of((PROPS, WINDOW)) + (first - off)
            pick = at == lax.broadcasted_iota(jnp.int32, (PROPS, WINDOW), 0)
            new = dot_tn(fresh_ref[s], jnp.where(pick, 1.0, 0.0).astype(bf16))[0:LINES]
            line = lanes_of((LINES, WINDOW)) + (first - off)
            old = buffer[s].astype(f32)
            buffer[s] = jnp.where((line >= 0) & (line < PROPS), new, old).astype(bf16)
            write(s, first).start()

        return carry

    def end(s, carry):
        _, hit, first = where_is(s)

        @pl.when(hit)
        def _():
            write(s, first).wait()

        return carry

    lax.fori_loop(0, SEQS, begin, 0)
    lax.fori_loop(0, SEQS, change, 0)
    lax.fori_loop(0, SEQS, end, 0)


def place(numbers, cache, fresh, so_far):
    return pl.pallas_call(
        place_kernel,
        out_shape=jax.ShapeDtypeStruct(cache.shape, cache.dtype),
        in_specs=[smem_spec(), any_spec(), vmem_spec(), any_spec()],
        out_specs=any_spec(),
        scratch_shapes=[
            VMEM((SEQS, LINES, WINDOW), bf16),
            pltpu.SemaphoreType.DMA((SEQS,)),
            pltpu.SemaphoreType.DMA((SEQS,)),
        ],
        input_output_aliases={3: 0},
        cost_estimate=cost(1e9, 2e6),
        compiler_params=pltpu.CompilerParams(vmem_limit_bytes=40 << 20),
        name="place",
    )(numbers, cache, fresh, so_far)


def ancestry(parents):
    _, prop_count = parents.shape
    slot_ids = jnp.arange(prop_count, dtype=jnp.int32)
    parent_links = (parents[:, :, None] == slot_ids[None, None, :]).astype(f32)
    identity = jnp.broadcast_to(jnp.eye(prop_count, dtype=f32), parent_links.shape)
    reached = jnp.minimum(identity + parent_links, 1.0)
    for _ in range((prop_count - 1).bit_length()):
        reached = jnp.minimum(
            jnp.einsum("sij,sjk->sik", reached, reached, precision=lax.Precision.HIGHEST), 1.0
        )
    depths = (jnp.sum(reached, axis=-1) - 1.0).astype(jnp.int32)
    return (reached, depths)


def exchange(value, axis):
    return lax.all_to_all(value, axis, 0, 0, tiled=True)


def layer(
    activations,
    latent_cache,
    lengths,
    accepted,
    parents,
    w_query_down,
    w_key_down,
    gain_input,
    gain_query,
    gain_key,
    w_query,
    w_value,
    w_out,
    gain_output,
):
    j = lax.axis_index("kv")
    t = lax.axis_index("tp")
    mine = t[None].astype(jnp.int32)
    cache = jnp.transpose(latent_cache, (0, 2, 1))

    x = pack(jnp.transpose(activations), w_query_down, w_key_down, gain_input[None])
    x = exchange(x, ALL).reshape(2048, 128)
    y = exchange(down(x), "tp")

    reached, depths = ancestry(parents)
    filled = lengths + accepted
    my_depths = lax.dynamic_slice_in_dim(depths, j, 1, 1)[:, 0]
    half = ROPE_DIM // 2
    frequency = ROPE_BASE ** (-jnp.arange(half, dtype=f32) / half)
    angles = (filled + my_depths).astype(f32)[:, None] * frequency[None, :]
    cosine, sine = jnp.cos(angles), jnp.sin(angles)
    nothing = jnp.zeros((SEQS, 96), f32)
    cosine = jnp.concatenate([cosine, cosine, nothing], axis=1)
    sine = jnp.concatenate([-sine, sine, nothing], axis=1)
    numbers = jnp.concatenate([filled - j * SPAN, t[None]]).astype(jnp.int32)
    group = lax.dynamic_index_in_dim(reached.reshape(3, 8, PROPS, PROPS), t, 1, False)
    anc = jnp.repeat(jnp.pad(group, ((0, 0), (0, 0), (0, 112))), 8, axis=1)

    wq = jnp.transpose(w_query, (1, 2, 0))
    wv = jnp.transpose(w_value, (0, 2, 1))
    z = queries(
        mine,
        y,
        gain_query.astype(f32).reshape(4, 128),
        gain_key.astype(f32).reshape(2, 128),
        cosine,
        sine,
        wq,
    )
    z = exchange(z, ALL)
    sent, fresh = attend(numbers, z, cache, anc, wv)

    updated = None
    for n in range(len(CUTS) - 1):
        updated = copy_cache(cache, updated, CUTS[n], CUTS[n + 1])
    updated = place(numbers, cache, fresh, updated)

    def shift(value, distance):
        return lax.ppermute(value, "tp", [(n, (n + distance) % 8) for n in range(8)])

    other = lax.ppermute(w_out, "tp", [(n, n ^ 1) for n in range(8)])
    w_here = [jnp.stack([w_out, other])]
    w_here += [shift(w_here[0], 2 * k) for k in range(1, 4)]
    attended = combine(exchange(sent, "kv"))
    mixed, squares = mix(mine, exchange(attended, "kv"), w_here)
    squares = exchange(squares, ALL).reshape(16, 8, 128)
    mixed = [mixed] + [shift(mixed, k) for k in range(1, 8)]
    result = finish(mine, squares, gain_output.astype(f32)[None], mixed)
    return (result, jnp.transpose(updated, (0, 2, 1)))


CUTS = (0, 5, 9, 24)


def solution(mesh):
    return jax.shard_map(
        layer,
        mesh=mesh,
        in_specs=(
            P(None, ALL),
            P(None, "kv", None),
            P(),
            P(),
            P(),
            P(ALL, None),
            P(ALL, None),
            P(ALL),
            P(),
            P(),
            P(None, "tp", None),
            P(),
            P("tp", "kv"),
            P("kv"),
        ),
        out_specs=(P(None, "kv"), P(None, "kv", None)),
        check_vma=False,
    )
```

```python
import jax
import jax.numpy as jnp
from jax import lax
from jax.experimental import pallas as pl
from jax.experimental.pallas import tpu as pltpu
from jax.sharding import Mesh
from jax.sharding import PartitionSpec as P


f32 = jnp.float32
bf16 = jnp.bfloat16

D = 2048
SEQS = 24
PROPS = 16
SPAN = 2048
KV_RANK = 256
ROPE_DIM = 32
LINES = 288
SCALE = 96.0 ** (-0.5)
EPS = 1e-06
ROPE_BASE = 10000.0
MASKED = -1e30
ALL = ("kv", "y", "c")
TP = ("y", "c")
CORES = ("kv", "c")
PLANES = ("kv", "y")
VMEM = pltpu.VMEM


def vmem_spec():
    return pl.BlockSpec(memory_space=pltpu.VMEM)


def smem_spec():
    return pl.BlockSpec(memory_space=pltpu.SMEM)


def any_spec():
    return pl.BlockSpec(memory_space=pl.ANY)


def cost(flops, moved):
    return pl.CostEstimate(flops=int(flops), bytes_accessed=int(moved), transcendentals=0)


def call(kernel, out_shape, inputs, price, scratch=(), limit=16):
    many = isinstance(out_shape, tuple)
    return pl.pallas_call(
        kernel,
        out_shape=out_shape,
        in_specs=[vmem_spec()] * inputs,
        out_specs=(vmem_spec(),) * len(out_shape) if many else vmem_spec(),
        scratch_shapes=list(scratch),
        cost_estimate=price,
        compiler_params=pltpu.CompilerParams(vmem_limit_bytes=limit << 20),
    )


def dot_nt(a, b):
    return lax.dot_general(a, b, (((1,), (1,)), ((), ())), preferred_element_type=f32)


def dot_nn(a, b):
    return lax.dot_general(a, b, (((1,), (0,)), ((), ())), preferred_element_type=f32)


def dot_tn(a, b):
    return lax.dot_general(a, b, (((0,), (0,)), ((), ())), preferred_element_type=f32)


def turn(v, n):
    return pltpu.roll(v, n % 128, v.ndim - 1)


def lanes_of(shape):
    return lax.broadcasted_iota(jnp.int32, shape, len(shape) - 1)


def rounded(v):
    return v.astype(bf16).astype(f32)


def pack_kernel(a_ref, q_ref, k_ref, g_ref, o_ref):
    row = lax.broadcasted_iota(jnp.int32, (384, 512), 0)
    place = (row & 15) * 32 + (row >> 4)
    pick = jnp.where(lanes_of((384, 512)) == place, 1.0, 0.0).astype(bf16)
    lines = dot_nn(a_ref[...], pick)
    lane = lanes_of((16, 128))
    gain = jnp.broadcast_to(g_ref[...].astype(f32), (16, 16))
    diagonal = lax.broadcasted_iota(jnp.int32, (16, 16), 0) == lanes_of((16, 16))
    gain = jnp.sum(jnp.where(diagonal, gain, 0.0), axis=1, keepdims=True)
    query = q_ref[...].astype(f32)
    key = k_ref[...].astype(f32)
    rope = jnp.concatenate([key[:, 256:288], jnp.zeros((16, 96), f32)], axis=1)
    columns = []
    for t in range(8):
        tile = query[:, (t // 2) * 128 : (t // 2) * 128 + 128]
        line = turn(tile, 24 - (t % 2) * 64)
        tile = key[:, (t // 4) * 128 : (t // 4) * 128 + 128]
        line = jnp.where(lane < 88, line, turn(tile, 88 - (t % 4) * 32))
        line = jnp.where(lane < 120, line, turn(rope, 120 - 4 * t))
        columns.append(jnp.where(lane < 124, line, jnp.where(lane == 124, gain, 0.0)))
    for j in range(16):
        tile = lines[:, (j // 4) * 128 : (j // 4) * 128 + 128]
        tile = turn(tile, -(j % 4) * 32) if j % 4 else tile
        for t in range(8):
            o_ref[j * 8 + t] = jnp.where(lane < 24, tile, columns[t]).astype(bf16)


def pack(a, q, k, g):
    return call(
        pack_kernel, jax.ShapeDtypeStruct((128, 16, 128), bf16), 4, cost(1e8, 1e6), limit=60
    )(a, q, k, g)


def down_kernel(x_ref, o_ref):
    x = x_ref[...]
    wide = x.astype(f32)
    lane = lanes_of(wide.shape)
    scaled = wide * wide[:, 124:125]
    lhs = jnp.where(lane < 24, scaled, turn(wide, 32)).astype(bf16)
    out = dot_tn(lhs, x)
    cross = out[32:56, :]
    row = lax.broadcasted_iota(jnp.int32, cross.shape, 0)
    squares = jnp.sum(jnp.where(row == lanes_of(cross.shape), cross, 0.0), axis=1, keepdims=True)
    o_ref[...] = jnp.broadcast_to(out[0:24, :] * lax.rsqrt(squares / D + EPS), o_ref.shape)


def down(x):
    return call(
        down_kernel,
        jax.ShapeDtypeStruct((8, 24, 128), f32),
        1,
        cost(2 * 128 * 128 * 2048, x.size * 2),
    )(x)


def query_kernel(t_ref, y_ref, gq_ref, gk_ref, cos_ref, sin_ref, w_ref, o_ref, block):
    mine = t_ref[0]
    lane = lanes_of((24, 128))
    parts = [y_ref[t] for t in range(8)]
    raw = [
        jnp.where(lane < 64, turn(parts[2 * a], -24), turn(parts[2 * a + 1], 40)) for a in range(4)
    ]
    squares = sum(jnp.sum(r * r, axis=1, keepdims=True) for r in raw)
    scale = lax.rsqrt(squares / 512.0 + EPS)
    low = jnp.concatenate(
        [raw[a] * scale * gq_ref[a : a + 1, :] for a in range(4)], axis=1
    ).astype(bf16)
    lats = []
    for half in range(2):
        lat = turn(parts[4 * half], -88)
        for u in range(1, 4):
            lat = jnp.where(lane >= u * 32, turn(parts[4 * half + u], u * 32 - 88), lat)
        lats.append(lat)
    squares = sum(jnp.sum(r * r, axis=1, keepdims=True) for r in lats)
    scale = lax.rsqrt(squares / 256.0 + EPS)
    lats = [rounded(lats[h] * scale * gk_ref[h : h + 1, :]) for h in range(2)]
    turned = turn(parts[0], -120)
    for t in range(1, 8):
        turned = jnp.where(lane >= 4 * t, turn(parts[t], 4 * t - 120), turned)
    cosine, sine = cos_ref[...], sin_ref[...]

    def rotate(v):
        partner = jnp.where(lane < 16, turn(v, -16), turn(v, 16))
        return v * cosine + partner * sine

    def own(tile):
        row = lax.broadcasted_iota(jnp.int32, tile.shape, 0)
        line = jnp.sum(jnp.where(row == mine, tile, 0.0), axis=0, keepdims=True)
        return jnp.broadcast_to(line, tile.shape)

    key_rope = rounded(rotate(turned))
    ropes = []
    query_rope = []
    for hh in range(2):
        lat = dot_nt(low, w_ref[hh, 0:256, :])
        rope = dot_nt(low, w_ref[hh, 256:288, :])
        rope = rotate(jnp.concatenate([rope, jnp.zeros((24, 96), f32)], axis=1))
        query_rope.append(rope)
        for s in range(3):
            for half in range(2):
                block[:, (s * 2 + hh) * 2 + half, :] = lat[
                    s * 8 : s * 8 + 8, half * 128 : half * 128 + 128
                ]
    for s in range(3):
        for half in range(2):
            block[:, 12 + s * 2 + half, :] = own(lats[half][s * 8 : s * 8 + 8, :])
    for s in range(3):
        for hh in range(2):
            ropes.append(query_rope[hh][s * 8 : s * 8 + 8, :])
    for s in range(3):
        ropes.append(own(key_rope[s * 8 : s * 8 + 8, :]))
    small = lanes_of((8, 128))
    for row in range(3):
        line = jnp.zeros((8, 128), f32)
        for n in range(4 * row, min(4 * row + 4, 9)):
            at = (n % 4) * 32
            line = jnp.where((small >= at) & (small < at + 32), turn(ropes[n], at), line)
        block[:, 18 + row, :] = line
        block[:, 21 + row, :] = jnp.zeros((8, 128), f32)
    packed = block[...].astype(bf16)
    for copy in range(16):
        o_ref[copy * 8 : copy * 8 + 8] = packed


def queries(mine, y, gq, gk, cosine, sine, w):
    return pl.pallas_call(
        query_kernel,
        out_shape=jax.ShapeDtypeStruct((128, 24, 128), bf16),
        in_specs=[smem_spec()] + [vmem_spec()] * 6,
        out_specs=vmem_spec(),
        scratch_shapes=[VMEM((8, 24, 128), f32)],
        cost_estimate=cost(2 * 24 * 512 * 576, 128 * 24 * 256),
        compiler_params=pltpu.CompilerParams(vmem_limit_bytes=16 << 20),
        name="queries",
    )(mine, y, gq, gk, cosine, sine, w)


CHUNK = 512
LOG2E = 1.4426950408889634


def attend_kernel(
    n_ref,
    z_ref,
    cache_ref,
    anc_ref,
    wv_ref,
    o_ref,
    fresh_ref,
    keys,
    wide,
    lines,
    part,
    lam,
    score,
    prob,
    sems,
):
    mine = n_ref[24]

    def fetch(s):
        return pltpu.make_async_copy(cache_ref.at[s * 8 + mine], keys.at[s], sems.at[s])

    for s in range(3):
        fetch(s).start()
    wide[...] = z_ref[...].astype(f32)
    lane = lanes_of((128, 128))
    packed = [wide[:, 18 + r, :] for r in range(3)]

    def rope_of(n):
        v = packed[n // 4]
        v = turn(v, -(n % 4) * 32) if n % 4 else v
        return jnp.where(lane < 32, v, 0.0)

    for s in range(3):
        for half in range(2):
            lines[s, half] = wide[:, 12 + s * 2 + half, :]
        lines[s, 2] = rope_of(6 + s)

    def fresh_of(s, t):
        return jnp.concatenate(
            [lines[s, a, pl.ds(t, 16, stride=8), :] for a in range(3)], axis=1
        ).astype(bf16)

    for s in range(3):
        for t in range(8):
            fresh_ref[s * 8 + t] = fresh_of(s, t)
    slot = lanes_of((256, 16))

    def tiles(v, join):
        out = v[:, 0:128]
        for n in range(1, v.shape[1] // 128):
            out = join(out, v[:, n * 128 : n * 128 + 128])
        return out

    def scores(s):
        off = n_ref[s * 8 + mine]
        fresh = fresh_of(s, mine)[:, 0:LINES]
        query = jnp.concatenate(
            [
                jnp.concatenate(
                    [
                        wide[:, (s * 2 + hh) * 2, :],
                        wide[:, (s * 2 + hh) * 2 + 1, :],
                        rope_of(s * 2 + hh)[:, 0:ROPE_DIM],
                    ],
                    axis=1,
                )
                for hh in range(2)
            ],
            axis=0,
        ).astype(bf16)
        near = dot_nt(query, fresh) * (SCALE * LOG2E)
        anc = anc_ref[s][:, 0:16]
        seen = (
            (jnp.concatenate([anc, anc], axis=0) > 0.5) & (slot + off >= 0) & (slot + off < SPAN)
        )
        near = jnp.where(seen, near, MASKED)
        most = None
        for c in range(SPAN // CHUNK):
            cols = slice(c * CHUNK, (c + 1) * CHUNK)
            bias = jnp.where(lanes_of((1, CHUNK)) + c * CHUNK < off, 0.0, MASKED)
            got = dot_nn(query, keys[s, :, cols]) * (SCALE * LOG2E) + bias
            score[s, :, cols] = got
            got = tiles(got, jnp.maximum)
            most = got if most is None else jnp.maximum(most, got)
        top = jnp.maximum(
            jnp.max(most, axis=1, keepdims=True), jnp.max(near, axis=1, keepdims=True)
        )
        return fresh, near, top

    def values(s, fresh, near, top):
        base = jnp.where(top < 0.1 * MASKED, 0.0, top)
        weight = jnp.exp2(near - base)
        total = jnp.sum(weight, axis=1, keepdims=True)
        acc = dot_nn(weight.astype(bf16), fresh[:, 0:KV_RANK])
        count = None
        for c in range(SPAN // CHUNK):
            cols = slice(c * CHUNK, (c + 1) * CHUNK)
            weight = jnp.exp2(score[s, :, cols] - base)
            prob[s, :, cols] = weight.astype(bf16)
            weight = tiles(weight, jnp.add)
            count = weight if count is None else count + weight
        total = total + jnp.sum(count, axis=1, keepdims=True)
        acc = acc + dot_nt(prob[s], keys[s, 0:KV_RANK, :])
        acc = rounded(acc / jnp.maximum(total, 1.0))
        for half in range(2):
            part[s, half] = acc[:, half * 128 : half * 128 + 128]
        level = jnp.where(total > 0.0, top + jnp.log2(jnp.maximum(total, 1.0)), MASKED)
        lam[s] = jnp.broadcast_to(level, (256, 128))

    fetch(0).wait()
    first = scores(0)
    fetch(1).wait()
    fetch(2).wait()
    second = scores(1)
    values(0, *first)
    third = scores(2)
    values(1, *second)
    values(2, *third)
    small = lanes_of((8, 128))
    short = lanes_of((24, 128))
    for quad in range(4):
        pieces, levels = [], []
        for h in range(4 * quad, 4 * quad + 4):
            level = jnp.zeros((8, 128), f32)
            for half in range(2):
                for s in range(3):
                    rows = pl.ds((h % 2) * 128 + half * 64 + h // 2, 8, stride=8)
                    pieces.append(
                        jnp.concatenate([part[s, a, rows, :] for a in range(2)], axis=1)
                    )
                    level = jnp.where(small // 4 == half * 3 + s, lam[s, rows, :], level)
            first = rounded(level)
            second = rounded(level - first)
            third = (level - first) - second
            level = jnp.where(small % 4 == 0, first, jnp.where(small % 4 == 1, second, third))
            levels.append(jnp.where(small % 4 == 3, 0.0, level))
        weights = wv_ref[4 * quad : 4 * quad + 4].reshape(256, 256)
        out = dot_nt(jnp.concatenate(pieces, axis=0).astype(bf16), weights)
        for a in range(4):
            tile = out[48 * a : 48 * a + 48, (a // 2) * 128 : (a // 2) * 128 + 128]
            low, high = tile[0:24], tile[24:48]
            if a % 2:
                tile = jnp.where(short < 64, turn(low, 64), high)
            else:
                tile = jnp.where(short < 64, low, turn(high, 64))
            o_ref[4 * quad + a] = jnp.concatenate([tile, levels[a]], axis=0).astype(bf16)


def attend(numbers, z, cache, anc, wv):
    return pl.pallas_call(
        attend_kernel,
        out_shape=(
            jax.ShapeDtypeStruct((16, 32, 128), bf16),
            jax.ShapeDtypeStruct((24, 16, 384), bf16),
        ),
        in_specs=[smem_spec(), vmem_spec(), any_spec(), vmem_spec(), vmem_spec()],
        out_specs=(vmem_spec(), vmem_spec()),
        scratch_shapes=[
            VMEM((3, LINES, SPAN), bf16),
            VMEM((128, 24, 128), f32),
            VMEM((3, 3, 128, 128), f32),
            VMEM((3, 2, 256, 128), f32),
            VMEM((3, 256, 128), f32),
            VMEM((3, 256, SPAN), f32),
            VMEM((3, 256, SPAN), bf16),
            pltpu.SemaphoreType.DMA((3,)),
        ],
        cost_estimate=cost(3 * 2 * 256 * 2048 * 544, 3 * LINES * SPAN * 2),
        compiler_params=pltpu.CompilerParams(vmem_limit_bytes=52 << 20),
        name="attend",
    )(numbers, z, cache, anc, wv)


def combine_kernel(v_ref, o_ref):
    v = v_ref[...].astype(f32)
    level = v[:, 24:32, :]
    level = (level + turn(level, -1)) + turn(level, -2)
    lane = lanes_of((16, 8, 128))
    outs = []
    for s in range(3):
        low, high = (level[:, :, 4 * (h * 3 + s) : 4 * (h * 3 + s) + 1] for h in range(2))
        both = jnp.where(lane < 64, low, high)
        share = jnp.exp2(both - jnp.max(both, axis=0, keepdims=True))
        summed = jnp.sum(share * v[:, s * 8 : s * 8 + 8, :], axis=0)
        outs.append(summed / jnp.sum(share, axis=0))
    o_ref[...] = jnp.broadcast_to(jnp.concatenate(outs, axis=0).astype(bf16), o_ref.shape)


def combine(v):
    return call(combine_kernel, jax.ShapeDtypeStruct((32, 24, 128), bf16), 1, cost(1e6, 1e5))(v)


def mix_kernel(t_ref, u_ref, *refs):
    w_refs, (o_ref, s_ref) = refs[:4], refs[4:]
    lane = lanes_of((24, 128))
    mixed = jnp.zeros((96, 128), f32)
    for k in range(4):
        for b in range(2):
            p = ((t_ref[0] - 2 * k) & 7) ^ b
            lhs = []
            for c in range(2):
                first, second = u_ref[2 * p, c].astype(f32), u_ref[2 * p + 1, c].astype(f32)
                lhs.append(jnp.where(lane < 64, first, turn(second, 64)))
                lhs.append(jnp.where(lane < 64, turn(first, 64), second))
            mixed = mixed + dot_nn(jnp.concatenate(lhs, axis=0).astype(bf16), w_refs[k][b])
    o_ref[...] = mixed
    squares = jnp.broadcast_to(jnp.sum(mixed * mixed, axis=1, keepdims=True), mixed.shape)
    row = lax.broadcasted_iota(jnp.int32, (96, 128), 0)
    line = jnp.sum(jnp.where(row == lanes_of((96, 128)), squares, 0.0), axis=0, keepdims=True)
    s_ref[...] = jnp.broadcast_to(line[None], s_ref.shape)


def mix(t, u, w):
    return pl.pallas_call(
        mix_kernel,
        out_shape=(
            jax.ShapeDtypeStruct((96, 128), f32),
            jax.ShapeDtypeStruct((64, 1, 128), f32),
        ),
        in_specs=[smem_spec()] + [vmem_spec()] * 5,
        out_specs=(vmem_spec(),) * 2,
        cost_estimate=cost(2 * 96 * 1024 * 128, 4e5),
        compiler_params=pltpu.CompilerParams(vmem_limit_bytes=16 << 20),
        name="mix",
    )(t, u, *w)


def finish_kernel(t_ref, s_ref, g_ref, *refs):
    m_refs, (o_ref, scale) = refs[:4], refs[4:]
    scale[...] = lax.rsqrt(jnp.sum(s_ref[...], axis=0) / D + EPS)
    row = lax.broadcasted_iota(jnp.int32, (96, 128), 0)
    same = row == lanes_of((96, 128))
    gain = g_ref[...]
    for k in range(4):
        y = ((t_ref[0] >> 1) - k) & 3
        inverse = scale[pl.ds(y, 1), :]
        column = jnp.sum(jnp.where(same, inverse, 0.0), axis=1, keepdims=True)
        out = m_refs[k][...] * column * gain
        for c in range(2):
            for s in range(3):
                at = c * 48 + s * 8
                rows = jnp.concatenate([out[at : at + 8], out[at + 24 : at + 32]], axis=0)
                at = pl.multiple_of((s * 8 + 2 * y + c) * 16, 16)
                o_ref[pl.ds(at, 16), :] = rows.astype(bf16)


def finish(t, s, g, m):
    return pl.pallas_call(
        finish_kernel,
        out_shape=jax.ShapeDtypeStruct((384, 128), bf16),
        in_specs=[smem_spec()] + [vmem_spec()] * 6,
        out_specs=vmem_spec(),
        scratch_shapes=[VMEM((4, 128), f32)],
        cost_estimate=cost(1e6, 4e5),
        compiler_params=pltpu.CompilerParams(vmem_limit_bytes=16 << 20),
        name="finish",
    )(t, s, g, *m)


DEPTH = 4


def copy_rows(source, target, buffer, into, outof, start, stop):
    count = stop - start

    def read(n, b):
        return pltpu.make_async_copy(source.at[start + n], buffer.at[b], into.at[b])

    def write(n, b):
        return pltpu.make_async_copy(buffer.at[b], target.at[start + n], outof.at[b])

    for n in range(min(DEPTH, count)):
        read(n, n).start()

    def body(n, carry):
        b = lax.rem(n, 2 * DEPTH)
        read(n, b).wait()
        write(n, b).start()

        @pl.when(n + DEPTH < count)
        def _():
            later = lax.rem(n + DEPTH, 2 * DEPTH)

            @pl.when(n >= DEPTH)
            def _():
                write(n - DEPTH, later).wait()

            read(n + DEPTH, later).start()

        return carry

    lax.fori_loop(0, count, body, 0)

    def drain(n, carry):
        write(n, lax.rem(n, 2 * DEPTH)).wait()
        return carry

    lax.fori_loop(max(0, count - 2 * DEPTH), count, drain, 0)


def copy_cache(cache, so_far, start, stop):
    def kernel(*refs):
        source = refs[0]
        target, buffer, into, outof = refs[-4:]
        copy_rows(source, target, buffer, into, outof, start, stop)

    first = so_far is None
    return pl.pallas_call(
        kernel,
        out_shape=jax.ShapeDtypeStruct(cache.shape, cache.dtype),
        in_specs=[any_spec()] * (1 if first else 2),
        out_specs=any_spec(),
        scratch_shapes=[
            VMEM((2 * DEPTH, LINES, SPAN), bf16),
            pltpu.SemaphoreType.DMA((2 * DEPTH,)),
            pltpu.SemaphoreType.DMA((2 * DEPTH,)),
        ],
        input_output_aliases={} if first else {1: 0},
        cost_estimate=cost((stop - start) * 9e8, (stop - start) * LINES * SPAN * 4),
        compiler_params=pltpu.CompilerParams(vmem_limit_bytes=40 << 20),
        name="copy_cache",
    )(*((cache,) if first else (cache, so_far)))


WINDOW = 256


def place_kernel(n_ref, cache_ref, fresh_ref, old_ref, o_ref, buffer, into, outof):
    def where_is(s):
        off = n_ref[s]
        hit = (off > -PROPS) & (off < SPAN)
        first = jnp.clip(off, 0, SPAN - 1)
        first = jnp.minimum((first // 128) * 128, SPAN - WINDOW)
        return off, hit, pl.multiple_of(first, 128)

    def read(s, first):
        return pltpu.make_async_copy(
            cache_ref.at[s, :, pl.ds(first, WINDOW)], buffer.at[s], into.at[s]
        )

    def write(s, first):
        return pltpu.make_async_copy(
            buffer.at[s], o_ref.at[s, :, pl.ds(first, WINDOW)], outof.at[s]
        )

    def begin(s, carry):
        _, hit, first = where_is(s)

        @pl.when(hit)
        def _():
            read(s, first).start()

        return carry

    def change(s, carry):
        off, hit, first = where_is(s)

        @pl.when(hit)
        def _():
            read(s, first).wait()
            at = lanes_of((PROPS, WINDOW)) + (first - off)
            pick = at == lax.broadcasted_iota(jnp.int32, (PROPS, WINDOW), 0)
            new = dot_tn(fresh_ref[s], jnp.where(pick, 1.0, 0.0).astype(bf16))[0:LINES]
            line = lanes_of((LINES, WINDOW)) + (first - off)
            old = buffer[s].astype(f32)
            buffer[s] = jnp.where((line >= 0) & (line < PROPS), new, old).astype(bf16)
            write(s, first).start()

        return carry

    def end(s, carry):
        _, hit, first = where_is(s)

        @pl.when(hit)
        def _():
            write(s, first).wait()

        return carry

    lax.fori_loop(0, SEQS, begin, 0)
    lax.fori_loop(0, SEQS, change, 0)
    lax.fori_loop(0, SEQS, end, 0)


def place(numbers, cache, fresh, so_far):
    return pl.pallas_call(
        place_kernel,
        out_shape=jax.ShapeDtypeStruct(cache.shape, cache.dtype),
        in_specs=[smem_spec(), any_spec(), vmem_spec(), any_spec()],
        out_specs=any_spec(),
        scratch_shapes=[
            VMEM((SEQS, LINES, WINDOW), bf16),
            pltpu.SemaphoreType.DMA((SEQS,)),
            pltpu.SemaphoreType.DMA((SEQS,)),
        ],
        input_output_aliases={3: 0},
        cost_estimate=cost(1e9, 2e6),
        compiler_params=pltpu.CompilerParams(vmem_limit_bytes=40 << 20),
        name="place",
    )(numbers, cache, fresh, so_far)


def ancestry(parents):
    _, prop_count = parents.shape
    slot_ids = jnp.arange(prop_count, dtype=jnp.int32)
    parent_links = (parents[:, :, None] == slot_ids[None, None, :]).astype(f32)
    identity = jnp.broadcast_to(jnp.eye(prop_count, dtype=f32), parent_links.shape)
    reached = jnp.minimum(identity + parent_links, 1.0)
    for _ in range((prop_count - 1).bit_length()):
        reached = jnp.minimum(
            jnp.einsum("sij,sjk->sik", reached, reached, precision=lax.Precision.HIGHEST), 1.0
        )
    depths = (jnp.sum(reached, axis=-1) - 1.0).astype(jnp.int32)
    return (reached, depths)


def exchange(value, axis):
    return lax.all_to_all(value, axis, 0, 0, tiled=True)


def layer(
    activations,
    latent_cache,
    lengths,
    accepted,
    parents,
    w_query_down,
    w_key_down,
    gain_input,
    gain_query,
    gain_key,
    w_query,
    w_value,
    w_out,
    gain_output,
):
    j = lax.axis_index("kv")
    t = lax.axis_index(TP)
    mine = t[None].astype(jnp.int32)
    cache = jnp.transpose(latent_cache, (0, 2, 1))

    x = pack(jnp.transpose(activations), w_query_down, w_key_down, gain_input[None])
    x = exchange(x, ALL).reshape(2048, 128)
    y = exchange(down(x), TP)

    reached, depths = ancestry(parents)
    filled = lengths + accepted
    my_depths = lax.dynamic_slice_in_dim(depths, j, 1, 1)[:, 0]
    half = ROPE_DIM // 2
    frequency = ROPE_BASE ** (-jnp.arange(half, dtype=f32) / half)
    angles = (filled + my_depths).astype(f32)[:, None] * frequency[None, :]
    cosine, sine = jnp.cos(angles), jnp.sin(angles)
    nothing = jnp.zeros((SEQS, 96), f32)
    cosine = jnp.concatenate([cosine, cosine, nothing], axis=1)
    sine = jnp.concatenate([-sine, sine, nothing], axis=1)
    numbers = jnp.concatenate([filled - j * SPAN, t[None]]).astype(jnp.int32)
    group = lax.dynamic_index_in_dim(reached.reshape(3, 8, PROPS, PROPS), t, 1, False)
    anc = jnp.repeat(jnp.pad(group, ((0, 0), (0, 0), (0, 112))), 8, axis=1)

    wq = jnp.transpose(w_query, (1, 2, 0))
    wv = jnp.transpose(w_value, (0, 2, 1))
    z = queries(
        mine,
        y,
        gain_query.astype(f32).reshape(4, 128),
        gain_key.astype(f32).reshape(2, 128),
        cosine,
        sine,
        wq,
    )
    z = exchange(z, ALL)
    other = lax.ppermute(w_out, TP, [(n, n ^ 1) for n in range(8)])
    z, other = lax.optimization_barrier((z, other))
    sent, fresh = attend(numbers, z, cache, anc, wv)

    updated = None
    for n in range(len(CUTS) - 1):
        updated = copy_cache(cache, updated, CUTS[n], CUTS[n + 1])
    updated = place(numbers, cache, fresh, updated)

    w_here = [jnp.stack([w_out, other])]
    w_here += [
        lax.ppermute(w_here[0], "y", [(n, (n + k) % 4) for n in range(4)]) for k in range(1, 4)
    ]
    sent = exchange(sent, "kv")
    attended = combine(sent)
    attended = exchange(attended, CORES).reshape(16, 2, 24, 128)
    mixed, squares = mix(mine, attended, w_here)
    squares = exchange(squares, PLANES).reshape(16, 4, 128)
    mixed = [mixed] + [
        lax.ppermute(mixed, "y", [(n, (n + k) % 4) for n in range(4)]) for k in range(1, 4)
    ]
    result = finish(mine, squares, gain_output.astype(f32)[None], mixed)
    return (result, jnp.transpose(updated, (0, 2, 1)))


CUTS = (0, 5, 9, 24)


def solution(mesh):
    split = Mesh(mesh.devices.reshape(16, 4, 2), ALL)
    return jax.shard_map(
        layer,
        mesh=split,
        in_specs=(
            P(None, ALL),
            P(None, "kv", None),
            P(),
            P(),
            P(),
            P(ALL, None),
            P(ALL, None),
            P(ALL),
            P(),
            P(),
            P(None, TP, None),
            P(),
            P(TP, "kv"),
            P("kv"),
        ),
        out_specs=(P(None, "kv"), P(None, "kv", None)),
        check_vma=False,
    )
```

```python
import jax
import jax.numpy as jnp
from jax import lax
from jax.experimental import pallas as pl
from jax.experimental.pallas import tpu as pltpu
from jax.sharding import Mesh
from jax.sharding import PartitionSpec as P


f32 = jnp.float32
bf16 = jnp.bfloat16

D = 2048
SEQS = 24
PROPS = 16
SPAN = 2048
KV_RANK = 256
ROPE_DIM = 32
LINES = 288
SCALE = 96.0 ** (-0.5)
EPS = 1e-06
ROPE_BASE = 10000.0
MASKED = -1e30
ALL = ("kv", "y", "c")
TP = ("y", "c")
CORES = ("kv", "c")
PLANES = ("kv", "y")
VMEM = pltpu.VMEM


def vmem_spec():
    return pl.BlockSpec(memory_space=pltpu.VMEM)


def smem_spec():
    return pl.BlockSpec(memory_space=pltpu.SMEM)


def any_spec():
    return pl.BlockSpec(memory_space=pl.ANY)


def cost(flops, moved):
    return pl.CostEstimate(flops=int(flops), bytes_accessed=int(moved), transcendentals=0)


def call(kernel, out_shape, inputs, price, scratch=(), limit=16):
    many = isinstance(out_shape, tuple)
    return pl.pallas_call(
        kernel,
        out_shape=out_shape,
        in_specs=[vmem_spec()] * inputs,
        out_specs=(vmem_spec(),) * len(out_shape) if many else vmem_spec(),
        scratch_shapes=list(scratch),
        cost_estimate=price,
        compiler_params=pltpu.CompilerParams(vmem_limit_bytes=limit << 20),
    )


def dot_nt(a, b):
    return lax.dot_general(a, b, (((1,), (1,)), ((), ())), preferred_element_type=f32)


def dot_nn(a, b):
    return lax.dot_general(a, b, (((1,), (0,)), ((), ())), preferred_element_type=f32)


def dot_tn(a, b):
    return lax.dot_general(a, b, (((0,), (0,)), ((), ())), preferred_element_type=f32)


def turn(v, n):
    return pltpu.roll(v, n % 128, v.ndim - 1)


def lanes_of(shape):
    return lax.broadcasted_iota(jnp.int32, shape, len(shape) - 1)


def rounded(v):
    return v.astype(bf16).astype(f32)


def pack_kernel(a_ref, q_ref, k_ref, g_ref, o_ref):
    row = lax.broadcasted_iota(jnp.int32, (384, 512), 0)
    place = (row & 15) * 32 + (row >> 4)
    pick = jnp.where(lanes_of((384, 512)) == place, 1.0, 0.0).astype(bf16)
    lines = dot_nn(a_ref[...], pick)
    lane = lanes_of((16, 128))
    gain = jnp.broadcast_to(g_ref[...].astype(f32), (16, 16))
    diagonal = lax.broadcasted_iota(jnp.int32, (16, 16), 0) == lanes_of((16, 16))
    gain = jnp.sum(jnp.where(diagonal, gain, 0.0), axis=1, keepdims=True)
    query = q_ref[...].astype(f32)
    key = k_ref[...].astype(f32)
    rope = jnp.concatenate([key[:, 256:288], jnp.zeros((16, 96), f32)], axis=1)
    columns = []
    for t in range(8):
        tile = query[:, (t // 2) * 128 : (t // 2) * 128 + 128]
        line = turn(tile, 24 - (t % 2) * 64)
        tile = key[:, (t // 4) * 128 : (t // 4) * 128 + 128]
        line = jnp.where(lane < 88, line, turn(tile, 88 - (t % 4) * 32))
        line = jnp.where(lane < 120, line, turn(rope, 120 - 4 * t))
        columns.append(jnp.where(lane < 124, line, jnp.where(lane == 124, gain, 0.0)))
    for j in range(16):
        tile = lines[:, (j // 4) * 128 : (j // 4) * 128 + 128]
        tile = turn(tile, -(j % 4) * 32) if j % 4 else tile
        for t in range(8):
            o_ref[j * 8 + t] = jnp.where(lane < 24, tile, columns[t]).astype(bf16)


def pack(a, q, k, g):
    return call(
        pack_kernel, jax.ShapeDtypeStruct((128, 16, 128), bf16), 4, cost(1e8, 1e6), limit=60
    )(a, q, k, g)


def down_kernel(x_ref, o_ref):
    x = x_ref[...]
    wide = x.astype(f32)
    lane = lanes_of(wide.shape)
    scaled = wide * wide[:, 124:125]
    lhs = jnp.where(lane < 24, scaled, turn(wide, 32)).astype(bf16)
    out = dot_tn(lhs, x)
    cross = out[32:56, :]
    row = lax.broadcasted_iota(jnp.int32, cross.shape, 0)
    squares = jnp.sum(jnp.where(row == lanes_of(cross.shape), cross, 0.0), axis=1, keepdims=True)
    o_ref[...] = jnp.broadcast_to(out[0:24, :] * lax.rsqrt(squares / D + EPS), o_ref.shape)


def down(x):
    return call(
        down_kernel,
        jax.ShapeDtypeStruct((8, 24, 128), f32),
        1,
        cost(2 * 128 * 128 * 2048, x.size * 2),
    )(x)


def query_kernel(t_ref, y_ref, gq_ref, gk_ref, cos_ref, sin_ref, w_ref, o_ref, block):
    mine = t_ref[0]
    lane = lanes_of((24, 128))
    parts = [y_ref[t] for t in range(8)]
    raw = [
        jnp.where(lane < 64, turn(parts[2 * a], -24), turn(parts[2 * a + 1], 40)) for a in range(4)
    ]
    squares = sum(jnp.sum(r * r, axis=1, keepdims=True) for r in raw)
    scale = lax.rsqrt(squares / 512.0 + EPS)
    low = jnp.concatenate(
        [raw[a] * scale * gq_ref[a : a + 1, :] for a in range(4)], axis=1
    ).astype(bf16)
    lats = []
    for half in range(2):
        lat = turn(parts[4 * half], -88)
        for u in range(1, 4):
            lat = jnp.where(lane >= u * 32, turn(parts[4 * half + u], u * 32 - 88), lat)
        lats.append(lat)
    squares = sum(jnp.sum(r * r, axis=1, keepdims=True) for r in lats)
    scale = lax.rsqrt(squares / 256.0 + EPS)
    lats = [rounded(lats[h] * scale * gk_ref[h : h + 1, :]) for h in range(2)]
    turned = turn(parts[0], -120)
    for t in range(1, 8):
        turned = jnp.where(lane >= 4 * t, turn(parts[t], 4 * t - 120), turned)
    cosine, sine = cos_ref[...], sin_ref[...]

    def rotate(v):
        partner = jnp.where(lane < 16, turn(v, -16), turn(v, 16))
        return v * cosine + partner * sine

    def own(tile):
        row = lax.broadcasted_iota(jnp.int32, tile.shape, 0)
        line = jnp.sum(jnp.where(row == mine, tile, 0.0), axis=0, keepdims=True)
        return jnp.broadcast_to(line, tile.shape)

    key_rope = rounded(rotate(turned))
    ropes = []
    query_rope = []
    for hh in range(2):
        lat = dot_nt(low, w_ref[hh, 0:256, :])
        rope = dot_nt(low, w_ref[hh, 256:288, :])
        rope = rotate(jnp.concatenate([rope, jnp.zeros((24, 96), f32)], axis=1))
        query_rope.append(rope)
        for s in range(3):
            for half in range(2):
                block[:, (s * 2 + hh) * 2 + half, :] = lat[
                    s * 8 : s * 8 + 8, half * 128 : half * 128 + 128
                ]
    for s in range(3):
        for half in range(2):
            block[:, 12 + s * 2 + half, :] = own(lats[half][s * 8 : s * 8 + 8, :])
    for s in range(3):
        for hh in range(2):
            ropes.append(query_rope[hh][s * 8 : s * 8 + 8, :])
    for s in range(3):
        ropes.append(own(key_rope[s * 8 : s * 8 + 8, :]))
    small = lanes_of((8, 128))
    for row in range(3):
        line = jnp.zeros((8, 128), f32)
        for n in range(4 * row, min(4 * row + 4, 9)):
            at = (n % 4) * 32
            line = jnp.where((small >= at) & (small < at + 32), turn(ropes[n], at), line)
        block[:, 18 + row, :] = line
        block[:, 21 + row, :] = jnp.zeros((8, 128), f32)
    packed = block[...].astype(bf16)
    for copy in range(16):
        o_ref[copy * 8 : copy * 8 + 8] = packed


def queries(mine, y, gq, gk, cosine, sine, w):
    return pl.pallas_call(
        query_kernel,
        out_shape=jax.ShapeDtypeStruct((128, 24, 128), bf16),
        in_specs=[smem_spec()] + [vmem_spec()] * 6,
        out_specs=vmem_spec(),
        scratch_shapes=[VMEM((8, 24, 128), f32)],
        cost_estimate=cost(2 * 24 * 512 * 576, 128 * 24 * 256),
        compiler_params=pltpu.CompilerParams(vmem_limit_bytes=16 << 20),
        name="queries",
    )(mine, y, gq, gk, cosine, sine, w)


CHUNK = 512
LOG2E = 1.4426950408889634


def keys_kernel(n_ref, cache_ref, o_ref, sems):
    mine = n_ref[24]

    def fetch(s):
        return pltpu.make_async_copy(cache_ref.at[s * 8 + mine], o_ref.at[s], sems.at[s])

    for s in range(3):
        fetch(s).start()
    for s in range(3):
        fetch(s).wait()


def own_keys(numbers, cache):
    return pl.pallas_call(
        keys_kernel,
        out_shape=jax.ShapeDtypeStruct((3, LINES, SPAN), bf16),
        in_specs=[smem_spec(), any_spec()],
        out_specs=vmem_spec(),
        scratch_shapes=[pltpu.SemaphoreType.DMA((3,))],
        cost_estimate=cost(1e8, 3 * LINES * SPAN * 4),
        compiler_params=pltpu.CompilerParams(vmem_limit_bytes=40 << 20),
        name="own_keys",
    )(numbers, cache)


def attend_kernel(
    n_ref,
    z_ref,
    keys,
    anc_ref,
    wv_ref,
    o_ref,
    fresh_ref,
    wide,
    lines,
    part,
    lam,
    score,
    prob,
):
    mine = n_ref[24]
    wide[...] = z_ref[...].astype(f32)
    lane = lanes_of((128, 128))
    packed = [wide[:, 18 + r, :] for r in range(3)]

    def rope_of(n):
        v = packed[n // 4]
        v = turn(v, -(n % 4) * 32) if n % 4 else v
        return jnp.where(lane < 32, v, 0.0)

    for s in range(3):
        for half in range(2):
            lines[s, half] = wide[:, 12 + s * 2 + half, :]
        lines[s, 2] = rope_of(6 + s)

    def fresh_of(s, t):
        return jnp.concatenate(
            [lines[s, a, pl.ds(t, 16, stride=8), :] for a in range(3)], axis=1
        ).astype(bf16)

    for s in range(3):
        for t in range(8):
            fresh_ref[s * 8 + t] = fresh_of(s, t)
    slot = lanes_of((256, 16))

    def tiles(v, join):
        out = v[:, 0:128]
        for n in range(1, v.shape[1] // 128):
            out = join(out, v[:, n * 128 : n * 128 + 128])
        return out

    def scores(s):
        off = n_ref[s * 8 + mine]
        fresh = fresh_of(s, mine)[:, 0:LINES]
        query = jnp.concatenate(
            [
                jnp.concatenate(
                    [
                        wide[:, (s * 2 + hh) * 2, :],
                        wide[:, (s * 2 + hh) * 2 + 1, :],
                        rope_of(s * 2 + hh)[:, 0:ROPE_DIM],
                    ],
                    axis=1,
                )
                for hh in range(2)
            ],
            axis=0,
        ).astype(bf16)
        near = dot_nt(query, fresh) * (SCALE * LOG2E)
        anc = anc_ref[s][:, 0:16]
        seen = (
            (jnp.concatenate([anc, anc], axis=0) > 0.5) & (slot + off >= 0) & (slot + off < SPAN)
        )
        near = jnp.where(seen, near, MASKED)
        most = None
        for c in range(SPAN // CHUNK):
            cols = slice(c * CHUNK, (c + 1) * CHUNK)
            bias = jnp.where(lanes_of((1, CHUNK)) + c * CHUNK < off, 0.0, MASKED)
            got = dot_nn(query, keys[s, :, cols]) * (SCALE * LOG2E) + bias
            score[s, :, cols] = got
            got = tiles(got, jnp.maximum)
            most = got if most is None else jnp.maximum(most, got)
        top = jnp.maximum(
            jnp.max(most, axis=1, keepdims=True), jnp.max(near, axis=1, keepdims=True)
        )
        return fresh, near, top

    def values(s, fresh, near, top):
        base = jnp.where(top < 0.1 * MASKED, 0.0, top)
        weight = jnp.exp2(near - base)
        total = jnp.sum(weight, axis=1, keepdims=True)
        acc = dot_nn(weight.astype(bf16), fresh[:, 0:KV_RANK])
        count = None
        for c in range(SPAN // CHUNK):
            cols = slice(c * CHUNK, (c + 1) * CHUNK)
            weight = jnp.exp2(score[s, :, cols] - base)
            prob[s, :, cols] = weight.astype(bf16)
            weight = tiles(weight, jnp.add)
            count = weight if count is None else count + weight
        total = total + jnp.sum(count, axis=1, keepdims=True)
        acc = acc + dot_nt(prob[s], keys[s, 0:KV_RANK, :])
        acc = rounded(acc / jnp.maximum(total, 1.0))
        for half in range(2):
            part[s, half] = acc[:, half * 128 : half * 128 + 128]
        level = jnp.where(total > 0.0, top + jnp.log2(jnp.maximum(total, 1.0)), MASKED)
        lam[s] = jnp.broadcast_to(level, (256, 128))

    first = scores(0)
    second = scores(1)
    values(0, *first)
    third = scores(2)
    values(1, *second)
    values(2, *third)
    small = lanes_of((8, 128))
    short = lanes_of((24, 128))
    for quad in range(4):
        pieces, levels = [], []
        for h in range(4 * quad, 4 * quad + 4):
            level = jnp.zeros((8, 128), f32)
            for half in range(2):
                for s in range(3):
                    rows = pl.ds((h % 2) * 128 + half * 64 + h // 2, 8, stride=8)
                    pieces.append(
                        jnp.concatenate([part[s, a, rows, :] for a in range(2)], axis=1)
                    )
                    level = jnp.where(small // 4 == half * 3 + s, lam[s, rows, :], level)
            first = rounded(level)
            second = rounded(level - first)
            third = (level - first) - second
            level = jnp.where(small % 4 == 0, first, jnp.where(small % 4 == 1, second, third))
            levels.append(jnp.where(small % 4 == 3, 0.0, level))
        weights = wv_ref[4 * quad : 4 * quad + 4].reshape(256, 256)
        out = dot_nt(jnp.concatenate(pieces, axis=0).astype(bf16), weights)
        for a in range(4):
            tile = out[48 * a : 48 * a + 48, (a // 2) * 128 : (a // 2) * 128 + 128]
            low, high = tile[0:24], tile[24:48]
            if a % 2:
                tile = jnp.where(short < 64, turn(low, 64), high)
            else:
                tile = jnp.where(short < 64, low, turn(high, 64))
            o_ref[4 * quad + a] = jnp.concatenate([tile, levels[a]], axis=0).astype(bf16)


def attend(numbers, z, keys, anc, wv):
    return pl.pallas_call(
        attend_kernel,
        out_shape=(
            jax.ShapeDtypeStruct((16, 32, 128), bf16),
            jax.ShapeDtypeStruct((24, 16, 384), bf16),
        ),
        in_specs=[smem_spec()] + [vmem_spec()] * 4,
        out_specs=(vmem_spec(), vmem_spec()),
        scratch_shapes=[
            VMEM((128, 24, 128), f32),
            VMEM((3, 3, 128, 128), f32),
            VMEM((3, 2, 256, 128), f32),
            VMEM((3, 256, 128), f32),
            VMEM((3, 256, SPAN), f32),
            VMEM((3, 256, SPAN), bf16),
        ],
        cost_estimate=cost(3 * 2 * 256 * 2048 * 544, 3 * LINES * SPAN * 2),
        compiler_params=pltpu.CompilerParams(vmem_limit_bytes=52 << 20),
        name="attend",
    )(numbers, z, keys, anc, wv)


def combine_kernel(v_ref, o_ref):
    v = v_ref[...].astype(f32)
    level = v[:, 24:32, :]
    level = (level + turn(level, -1)) + turn(level, -2)
    lane = lanes_of((16, 8, 128))
    outs = []
    for s in range(3):
        low, high = (level[:, :, 4 * (h * 3 + s) : 4 * (h * 3 + s) + 1] for h in range(2))
        both = jnp.where(lane < 64, low, high)
        share = jnp.exp2(both - jnp.max(both, axis=0, keepdims=True))
        summed = jnp.sum(share * v[:, s * 8 : s * 8 + 8, :], axis=0)
        outs.append(summed / jnp.sum(share, axis=0))
    o_ref[...] = jnp.broadcast_to(jnp.concatenate(outs, axis=0).astype(bf16), o_ref.shape)


def combine(v):
    return call(combine_kernel, jax.ShapeDtypeStruct((32, 24, 128), bf16), 1, cost(1e6, 1e5))(v)


def mix_kernel(t_ref, u_ref, *refs):
    w_refs, (o_ref, s_ref) = refs[:4], refs[4:]
    lane = lanes_of((24, 128))
    mixed = jnp.zeros((96, 128), f32)
    for k in range(4):
        for b in range(2):
            p = ((t_ref[0] - 2 * k) & 7) ^ b
            lhs = []
            for c in range(2):
                first, second = u_ref[2 * p, c].astype(f32), u_ref[2 * p + 1, c].astype(f32)
                lhs.append(jnp.where(lane < 64, first, turn(second, 64)))
                lhs.append(jnp.where(lane < 64, turn(first, 64), second))
            mixed = mixed + dot_nn(jnp.concatenate(lhs, axis=0).astype(bf16), w_refs[k][b])
    o_ref[...] = mixed
    squares = jnp.broadcast_to(jnp.sum(mixed * mixed, axis=1, keepdims=True), mixed.shape)
    row = lax.broadcasted_iota(jnp.int32, (96, 128), 0)
    line = jnp.sum(jnp.where(row == lanes_of((96, 128)), squares, 0.0), axis=0, keepdims=True)
    s_ref[...] = jnp.broadcast_to(line[None], s_ref.shape)


def mix(t, u, w):
    return pl.pallas_call(
        mix_kernel,
        out_shape=(
            jax.ShapeDtypeStruct((96, 128), f32),
            jax.ShapeDtypeStruct((64, 1, 128), f32),
        ),
        in_specs=[smem_spec()] + [vmem_spec()] * 5,
        out_specs=(vmem_spec(),) * 2,
        cost_estimate=cost(2 * 96 * 1024 * 128, 4e5),
        compiler_params=pltpu.CompilerParams(vmem_limit_bytes=16 << 20),
        name="mix",
    )(t, u, *w)


def finish_kernel(t_ref, s_ref, g_ref, *refs):
    m_refs, (o_ref, scale) = refs[:4], refs[4:]
    scale[...] = lax.rsqrt(jnp.sum(s_ref[...], axis=0) / D + EPS)
    row = lax.broadcasted_iota(jnp.int32, (96, 128), 0)
    same = row == lanes_of((96, 128))
    gain = g_ref[...]
    for k in range(4):
        y = ((t_ref[0] >> 1) - k) & 3
        inverse = scale[pl.ds(y, 1), :]
        column = jnp.sum(jnp.where(same, inverse, 0.0), axis=1, keepdims=True)
        out = m_refs[k][...] * column * gain
        for c in range(2):
            for s in range(3):
                at = c * 48 + s * 8
                rows = jnp.concatenate([out[at : at + 8], out[at + 24 : at + 32]], axis=0)
                at = pl.multiple_of((s * 8 + 2 * y + c) * 16, 16)
                o_ref[pl.ds(at, 16), :] = rows.astype(bf16)


def finish(t, s, g, m):
    return pl.pallas_call(
        finish_kernel,
        out_shape=jax.ShapeDtypeStruct((384, 128), bf16),
        in_specs=[smem_spec()] + [vmem_spec()] * 6,
        out_specs=vmem_spec(),
        scratch_shapes=[VMEM((4, 128), f32)],
        cost_estimate=cost(1e6, 4e5),
        compiler_params=pltpu.CompilerParams(vmem_limit_bytes=16 << 20),
        name="finish",
    )(t, s, g, *m)


DEPTH = 4


def copy_rows(source, target, buffer, into, outof, start, stop):
    count = stop - start

    def read(n, b):
        return pltpu.make_async_copy(source.at[start + n], buffer.at[b], into.at[b])

    def write(n, b):
        return pltpu.make_async_copy(buffer.at[b], target.at[start + n], outof.at[b])

    for n in range(min(DEPTH, count)):
        read(n, n).start()

    def body(n, carry):
        b = lax.rem(n, 2 * DEPTH)
        read(n, b).wait()
        write(n, b).start()

        @pl.when(n + DEPTH < count)
        def _():
            later = lax.rem(n + DEPTH, 2 * DEPTH)

            @pl.when(n >= DEPTH)
            def _():
                write(n - DEPTH, later).wait()

            read(n + DEPTH, later).start()

        return carry

    lax.fori_loop(0, count, body, 0)

    def drain(n, carry):
        write(n, lax.rem(n, 2 * DEPTH)).wait()
        return carry

    lax.fori_loop(max(0, count - 2 * DEPTH), count, drain, 0)


def copy_cache(cache, so_far, start, stop):
    def kernel(*refs):
        source = refs[0]
        target, buffer, into, outof = refs[-4:]
        copy_rows(source, target, buffer, into, outof, start, stop)

    first = so_far is None
    return pl.pallas_call(
        kernel,
        out_shape=jax.ShapeDtypeStruct(cache.shape, cache.dtype),
        in_specs=[any_spec()] * (1 if first else 2),
        out_specs=any_spec(),
        scratch_shapes=[
            VMEM((2 * DEPTH, LINES, SPAN), bf16),
            pltpu.SemaphoreType.DMA((2 * DEPTH,)),
            pltpu.SemaphoreType.DMA((2 * DEPTH,)),
        ],
        input_output_aliases={} if first else {1: 0},
        cost_estimate=cost((stop - start) * 9e8, (stop - start) * LINES * SPAN * 4),
        compiler_params=pltpu.CompilerParams(vmem_limit_bytes=40 << 20),
        name="copy_cache",
    )(*((cache,) if first else (cache, so_far)))


WINDOW = 256


def place_kernel(n_ref, cache_ref, fresh_ref, old_ref, o_ref, buffer, into, outof):
    def where_is(s):
        off = n_ref[s]
        hit = (off > -PROPS) & (off < SPAN)
        first = jnp.clip(off, 0, SPAN - 1)
        first = jnp.minimum((first // 128) * 128, SPAN - WINDOW)
        return off, hit, pl.multiple_of(first, 128)

    def read(s, first):
        return pltpu.make_async_copy(
            cache_ref.at[s, :, pl.ds(first, WINDOW)], buffer.at[s], into.at[s]
        )

    def write(s, first):
        return pltpu.make_async_copy(
            buffer.at[s], o_ref.at[s, :, pl.ds(first, WINDOW)], outof.at[s]
        )

    def begin(s, carry):
        _, hit, first = where_is(s)

        @pl.when(hit)
        def _():
            read(s, first).start()

        return carry

    def change(s, carry):
        off, hit, first = where_is(s)

        @pl.when(hit)
        def _():
            read(s, first).wait()
            at = lanes_of((PROPS, WINDOW)) + (first - off)
            pick = at == lax.broadcasted_iota(jnp.int32, (PROPS, WINDOW), 0)
            new = dot_tn(fresh_ref[s], jnp.where(pick, 1.0, 0.0).astype(bf16))[0:LINES]
            line = lanes_of((LINES, WINDOW)) + (first - off)
            old = buffer[s].astype(f32)
            buffer[s] = jnp.where((line >= 0) & (line < PROPS), new, old).astype(bf16)
            write(s, first).start()

        return carry

    def end(s, carry):
        _, hit, first = where_is(s)

        @pl.when(hit)
        def _():
            write(s, first).wait()

        return carry

    lax.fori_loop(0, SEQS, begin, 0)
    lax.fori_loop(0, SEQS, change, 0)
    lax.fori_loop(0, SEQS, end, 0)


def place(numbers, cache, fresh, so_far):
    return pl.pallas_call(
        place_kernel,
        out_shape=jax.ShapeDtypeStruct(cache.shape, cache.dtype),
        in_specs=[smem_spec(), any_spec(), vmem_spec(), any_spec()],
        out_specs=any_spec(),
        scratch_shapes=[
            VMEM((SEQS, LINES, WINDOW), bf16),
            pltpu.SemaphoreType.DMA((SEQS,)),
            pltpu.SemaphoreType.DMA((SEQS,)),
        ],
        input_output_aliases={3: 0},
        cost_estimate=cost(1e9, 2e6),
        compiler_params=pltpu.CompilerParams(vmem_limit_bytes=40 << 20),
        name="place",
    )(numbers, cache, fresh, so_far)


def ancestry(parents):
    _, prop_count = parents.shape
    slot_ids = jnp.arange(prop_count, dtype=jnp.int32)
    parent_links = (parents[:, :, None] == slot_ids[None, None, :]).astype(f32)
    identity = jnp.broadcast_to(jnp.eye(prop_count, dtype=f32), parent_links.shape)
    reached = jnp.minimum(identity + parent_links, 1.0)
    for _ in range((prop_count - 1).bit_length()):
        reached = jnp.minimum(
            jnp.einsum("sij,sjk->sik", reached, reached, precision=lax.Precision.HIGHEST), 1.0
        )
    depths = (jnp.sum(reached, axis=-1) - 1.0).astype(jnp.int32)
    return (reached, depths)


def exchange(value, axis):
    return lax.all_to_all(value, axis, 0, 0, tiled=True)


def layer(
    activations,
    latent_cache,
    lengths,
    accepted,
    parents,
    w_query_down,
    w_key_down,
    gain_input,
    gain_query,
    gain_key,
    w_query,
    w_value,
    w_out,
    gain_output,
):
    j = lax.axis_index("kv")
    t = lax.axis_index(TP)
    mine = t[None].astype(jnp.int32)
    cache = jnp.transpose(latent_cache, (0, 2, 1))

    x = pack(jnp.transpose(activations), w_query_down, w_key_down, gain_input[None])
    x = exchange(x, ALL).reshape(2048, 128)
    y = exchange(down(x), TP)

    reached, depths = ancestry(parents)
    filled = lengths + accepted
    my_depths = lax.dynamic_slice_in_dim(depths, j, 1, 1)[:, 0]
    half = ROPE_DIM // 2
    frequency = ROPE_BASE ** (-jnp.arange(half, dtype=f32) / half)
    angles = (filled + my_depths).astype(f32)[:, None] * frequency[None, :]
    cosine, sine = jnp.cos(angles), jnp.sin(angles)
    nothing = jnp.zeros((SEQS, 96), f32)
    cosine = jnp.concatenate([cosine, cosine, nothing], axis=1)
    sine = jnp.concatenate([-sine, sine, nothing], axis=1)
    numbers = jnp.concatenate([filled - j * SPAN, t[None]]).astype(jnp.int32)
    group = lax.dynamic_index_in_dim(reached.reshape(3, 8, PROPS, PROPS), t, 1, False)
    anc = jnp.repeat(jnp.pad(group, ((0, 0), (0, 0), (0, 112))), 8, axis=1)

    wq = jnp.transpose(w_query, (1, 2, 0))
    wv = jnp.transpose(w_value, (0, 2, 1))
    z = queries(
        mine,
        y,
        gain_query.astype(f32).reshape(4, 128),
        gain_key.astype(f32).reshape(2, 128),
        cosine,
        sine,
        wq,
    )
    z = exchange(z, ALL)
    other = lax.ppermute(w_out, TP, [(n, n ^ 1) for n in range(8)])
    z, other = lax.optimization_barrier((z, other))
    keys = own_keys(numbers, cache)
    sent, fresh = attend(numbers, z, keys, anc, wv)

    updated = None
    for n in range(len(CUTS) - 1):
        updated = copy_cache(cache, updated, CUTS[n], CUTS[n + 1])
    updated = place(numbers, cache, fresh, updated)

    w_here = [jnp.stack([w_out, other])]
    w_here += [
        lax.ppermute(w_here[0], "y", [(n, (n + k) % 4) for n in range(4)]) for k in range(1, 4)
    ]
    sent = exchange(sent, "kv")
    attended = combine(sent)
    attended = exchange(attended, CORES).reshape(16, 2, 24, 128)
    mixed, squares = mix(mine, attended, w_here)
    squares = exchange(squares, PLANES).reshape(16, 4, 128)
    mixed = [mixed] + [
        lax.ppermute(mixed, "y", [(n, (n + k) % 4) for n in range(4)]) for k in range(1, 4)
    ]
    result = finish(mine, squares, gain_output.astype(f32)[None], mixed)
    return (result, jnp.transpose(updated, (0, 2, 1)))


CUTS = (0, 6, 11, 24)


def solution(mesh):
    split = Mesh(mesh.devices.reshape(16, 4, 2), ALL)
    return jax.shard_map(
        layer,
        mesh=split,
        in_specs=(
            P(None, ALL),
            P(None, "kv", None),
            P(),
            P(),
            P(),
            P(ALL, None),
            P(ALL, None),
            P(ALL),
            P(),
            P(),
            P(None, TP, None),
            P(),
            P(TP, "kv"),
            P("kv"),
        ),
        out_specs=(P(None, "kv"), P(None, "kv", None)),
        check_vma=False,
    )
```
